256 devices in a mesh: grp: 2 (over y), ep: 32 (over z, core), tp: 4 (over x).
Axes of the slice: x: 4, y: 2, z: 16, core: 2. Of those that a mesh axis runs over, the one named last changes fastest.
The devices are a block of a 4x16x16 slice.
Arguments:
- mixer_tokens: bfloat16 [32768, 2048], P(('grp', 'ep', 'tp')), parts along dimension 0, may hold values from -6 to 6
- mixer_gain: bfloat16 [2048], replicated, may hold values from 0.099609375 to 1.8984375
- in_weight: bfloat16 [2048, 2048], P(None, 'tp'), may hold values from -0.125 to 0.125
- group_weight: bfloat16 [4, 512, 512], P('tp'), may hold values from -0.25 to 0.25
- channel_scale: bfloat16 [2048], P('tp'), may hold values from 0.099609375 to 1.8984375
- out_weight: bfloat16 [2048, 2048], P('tp'), may hold values from -0.125 to 0.125
- expert_tokens: bfloat16 [32768, 2048], P(('grp', 'ep', 'tp')), parts along dimension 0, may hold values from -6 to 6
- expert_gain: bfloat16 [2048], replicated, may hold values from 0.099609375 to 1.8984375
- route_ids: int32 [32768, 2], P(('grp', 'ep', 'tp')), parts along dimension 0, may hold values from 0 to 31, all different within a row; in each aligned block of 128 rows (0 to 127, 128 to 255, ...) at most 16 rows name the same one
- route_weights: float32 [32768, 2], P(('grp', 'ep', 'tp')), parts along dimension 0, may hold values from 0.1 to 1
- gate_weight: bfloat16 [32, 2048, 1024], P('ep', None, 'tp'), may hold values from -0.125 to 0.125
- up_weight: bfloat16 [32, 2048, 1024], P('ep', None, 'tp'), may hold values from -0.125 to 0.125
- down_weight: bfloat16 [32, 1024, 2048], P('ep', 'tp'), may hold values from -0.1875 to 0.1875
Outputs:
- mixed_tokens: bfloat16 [32768, 2048], P(('grp', 'ep', 'tp')), parts along dimension 0
- expert_mix: bfloat16 [32768, 2048], P(('grp', 'ep', 'tp')), parts along dimension 0
The draws below stay inside these ranges and needn't reach their ends.
There are 2 independent parts, one for each index of `grp`. The reference program is written for one: setup_inputs(seed, part) draws one part's arguments, and reference() takes and returns one part's arrays. A program takes and returns all parts, laid end to end along the dimension named above; an argument that names none is the same for every part. Nothing has to cross between parts.
Inputs may be any that keep to these rules, and one draw needn't show every extreme that they name: `route_ids`: each row names 2 different experts; in the rows of one device no expert is named more than 16 times, and one expert exactly 16 times in the rows of some device.
All inputs are finite; a program needn't handle non-finite values.
Results may differ from the reference program's by a relative error of at most 0.015.
Values may be sent and summed in bfloat16 or wider, within the bound.
No kernel may reach another device: no remote copies, remote signals or barrier semaphores. Data moves between devices by JAX's collectives and lax.ppermute only.
A program may use at most 128 MiB of HBM per device.

```python
import math
import jax
import jax.numpy as jnp
import numpy as np
from jax import lax

D = 2048
GROUPS = 4
GW = 512
FF = 1024
FF_DEV = 256
TOP = 2
TOK_DEV = 128
TOKENS = 16384
EXPERTS = 32
CAP = 16
N_EP = 32
N_TP = 4


def block_levels(key, dims, split, least, high):
    def one(position, shards_of):
        heights = jax.random.uniform(jax.random.fold_in(jax.random.fold_in(key, 6), position), (shards_of,), jnp.float32, least / len(split), high / len(split))
        return jnp.repeat(jnp.exp(heights), dims[position] // shards_of).reshape((-1,) + (1,) * (len(dims) - position - 1))

    level = one(*split[0])
    for cut in split[1:]:
        level = level * one(*cut)
    return level


def routed_block(own_key, own, number, rows, number_of, top, bound, lean):
    order = jax.random.permutation(own_key, number_of)
    heavy_load, ordinary = portions_of(number_of, rows * top, bound, lean, True), portions_of(number_of, rows * top, bound, lean, False)
    places = jnp.arange(number_of)

    def named(lengths, rotation):
        used = int((lengths > 0).sum())
        fixed = max(1, used // 4)
        moved = fixed + (places - fixed + rotation * (used - fixed)) % max(1, number_of - fixed)
        return jnp.zeros((number_of,), jnp.int32).at[order[jnp.where(places < fixed, places, moved)]].set(jnp.asarray(lengths, jnp.int32))

    lengths = jnp.where(number % 4 == 0, named(heavy_load, number // 4), named(ordinary, number - number // 4 - 1))
    mixed = jax.random.permutation(jax.random.fold_in(own, 3), number_of)
    source_of, taker = mixed[0:number_of // 2 * 2:2], mixed[1:number_of // 2 * 2:2]
    room = jnp.minimum(lengths[source_of] - 1, bound - lengths[taker]) // 2
    room = jnp.where((source_of == order[0]) | (taker == order[0]) | (lengths[taker] == 0), 0, jnp.maximum(room, 0))
    moved = jax.random.randint(jax.random.fold_in(own, 4), (number_of // 2,), 0, 1 << 20) % (room + 1)
    lengths = lengths.at[source_of].add(-moved).at[taker].add(moved)
    labels = jnp.searchsorted(jnp.cumsum(lengths), jnp.arange(rows * top), side="right").astype(jnp.int32)
    listing = labels.reshape(top, rows).T
    listing = listing[jax.random.permutation(jax.random.fold_in(own, 1), rows)]
    rotation = jax.random.randint(jax.random.fold_in(own, 2), (rows, 1), 0, top)
    return jnp.take_along_axis(listing, (jnp.arange(top)[None, :] + rotation) % top, axis=1)


def portions_of(number_of, total, most, lean, full):
    loads = [(1 << 20) // math.isqrt(rank ** lean) + 1 for rank in range(1, number_of + 1)]
    largest = most if full else min(most, max(-(-total // number_of), total * loads[0] // sum(loads)))
    least = 1 if total - largest >= number_of - 1 else 0
    holding, spare = [largest] + [least] * (number_of - 1), total - largest - least * (number_of - 1)
    while spare > 0:
        free = [i for i in range(1, number_of) if holding[i] < largest] or [i for i in range(1, number_of) if holding[i] < most]
        pool, budget = sum([loads[i] for i in free]), spare
        for i in free:
            more = min(most - holding[i], max(1, budget * loads[i] // pool), spare)
            holding[i] = holding[i] + more
            spare = spare - more
    return np.array(holding)


def bell_draw(key, shape, scale, bound, split=(), kind=jnp.bfloat16):
    entries = jax.random.normal(key, shape, jnp.float32) * scale
    if len(split) > 0:
        entries = block_levels(key, shape, split, -0.22, 0.18) * entries
    return jnp.clip(entries, min=-bound, max=bound).astype(kind)


def setup_inputs(seed: int = 0, part: int = 0) -> dict:
    splits = jax.random.split(jax.random.key(seed), 14)
    part_keys = jax.random.split(jax.random.fold_in(splits[13], part), 14)
    mixer_tokens = bell_draw(part_keys[0], (TOKENS, D), 1.0, 6.0, ((0, 128),))
    mixer_gain = jnp.clip(1.0 + 0.18 * jax.random.normal(splits[1], (D,), jnp.float32), 0.099609375, 1.8984375).astype(jnp.bfloat16)
    in_weight = bell_draw(splits[2], (D, D), D ** -0.5, 0.125, ((1, 4),))
    group_weight = bell_draw(splits[3], (GROUPS, GW, GW), GW ** -0.5, 0.25, ((0, 4),))
    channel_scale = jnp.clip(1.0 + 0.18 * jax.random.normal(splits[4], (D,), jnp.float32), 0.099609375, 1.8984375).astype(jnp.bfloat16)
    out_weight = bell_draw(splits[5], (D, D), D ** -0.5, 0.125, ((0, 4),))
    expert_tokens = bell_draw(part_keys[6], (TOKENS, D), 1.0, 6.0, ((0, 128),))
    expert_gain = jnp.clip(1.0 + 0.18 * jax.random.normal(splits[7], (D,), jnp.float32), 0.099609375, 1.8984375).astype(jnp.bfloat16)
    route_ids_keys = jax.random.split(jax.random.fold_in(part_keys[8], 1), TOKENS // TOK_DEV)
    route_ids_turns = jax.random.permutation(jax.random.fold_in(part_keys[8], 3), TOKENS // TOK_DEV)
    route_ids = jax.vmap(lambda own, number: routed_block(jax.random.fold_in(part_keys[8], 2), own, number, TOK_DEV, EXPERTS, TOP, CAP, 2))(route_ids_keys, route_ids_turns).reshape((TOKENS, TOP))
    route_weights = jnp.clip(jnp.exp(math.log(1.0) - 2.3025851 * jax.random.uniform(part_keys[9], (TOKENS, TOP), jnp.float32) ** block_levels(part_keys[9], (TOKENS, TOP), ((0, 128),), -0.2, 0.2)), 0.1, 1.0)
    gate_weight = bell_draw(splits[10], (EXPERTS, D, FF), D ** -0.5, 0.125, ((0, 32), (2, 4)))
    up_weight = bell_draw(splits[11], (EXPERTS, D, FF), D ** -0.5, 0.125, ((0, 32), (2, 4)))
    down_weight = bell_draw(splits[12], (EXPERTS, FF, D), FF ** -0.5, 0.1875, ((0, 32), (1, 4)))
    return dict(mixer_tokens=mixer_tokens, mixer_gain=mixer_gain, in_weight=in_weight, group_weight=group_weight, channel_scale=channel_scale, out_weight=out_weight, expert_tokens=expert_tokens, expert_gain=expert_gain, route_ids=route_ids, route_weights=route_weights, gate_weight=gate_weight, up_weight=up_weight, down_weight=down_weight)


def rms_rows(rows, gain):
    values = rows.astype(jnp.float32)
    scaled = values * lax.rsqrt(lax.optimization_barrier(jnp.mean(values * values, axis=-1, keepdims=True)) + 1e-06)
    return (scaled * gain.astype(jnp.float32)).astype(jnp.bfloat16)

def expert_hidden(rows, w_gate, w_up):
    gate = jnp.dot(rows, w_gate, preferred_element_type=jnp.float32)
    upper = jnp.dot(rows, w_up, preferred_element_type=jnp.float32)
    return (jax.nn.silu(gate) * upper).astype(jnp.bfloat16)

def reference(mixer_tokens, mixer_gain, in_weight, group_weight, channel_scale, out_weight, expert_tokens, expert_gain, route_ids, route_weights, gate_weight, up_weight, down_weight):
    normed = rms_rows(mixer_tokens, mixer_gain)
    pooled_in = jnp.dot(normed, in_weight, preferred_element_type=jnp.float32).astype(jnp.bfloat16)
    values = pooled_in.astype(jnp.float32)
    length = values.shape[0]
    prefix = jnp.concatenate([jnp.zeros((1, D), jnp.float32), jnp.cumsum(values, axis=0)], axis=0)
    mixed = jnp.zeros((length, D), jnp.float32)
    for group in range(GROUPS):
        window = 2 ** (group + 1)
        low_col = group * GW
        upper = prefix[1:, low_col:low_col + GW]
        lower = jnp.concatenate([jnp.zeros((window - 1, GW), jnp.float32), prefix[:length - window + 1, low_col:low_col + GW]], axis=0)
        counts = jnp.minimum(jnp.arange(1, length + 1), window).astype(jnp.float32)
        trail = ((upper - lower) / counts[:, None] - values[:, low_col:low_col + GW]).astype(jnp.bfloat16)
        grouped = (jnp.dot(trail, group_weight[group], preferred_element_type=jnp.float32) * channel_scale[low_col:low_col + GW].astype(jnp.float32)).astype(jnp.bfloat16)
        partial_value = jnp.dot(grouped, out_weight[low_col:low_col + GW, :], preferred_element_type=jnp.float32)
        partial_value = lax.optimization_barrier(partial_value.astype(jnp.bfloat16))
        mixed = mixed + partial_value.astype(jnp.float32)
    mixed_tokens = mixed.astype(jnp.bfloat16)
    expert_in = rms_rows(expert_tokens, expert_gain)
    weights = route_weights.astype(jnp.float32)
    shares = weights / lax.optimization_barrier(jnp.sum(weights, axis=1, keepdims=True))
    count_tok = expert_in.shape[0]
    flat_ids = route_ids.reshape(count_tok * TOP).astype(jnp.int32)
    flat_tokens = jnp.concatenate([(jnp.arange(count_tok * TOP) // TOP).astype(jnp.int32), jnp.full((1,), count_tok, jnp.int32)])
    flat_shares = jnp.concatenate([shares.reshape(count_tok * TOP), jnp.zeros((1,), jnp.float32)])
    padded = jnp.concatenate([expert_in, jnp.zeros((1, D), jnp.bfloat16)], axis=0)
    most = N_EP * N_TP * CAP

    def one_expert(total, expert):
        chosen = jnp.nonzero(flat_ids == expert, size=most, fill_value=count_tok * TOP)[0].astype(jnp.int32)
        token_of = flat_tokens[chosen]
        rows = padded[token_of]
        hidden = expert_hidden(rows, gate_weight[expert], up_weight[expert])
        result = jnp.zeros((most, D), jnp.float32)
        for block in range(N_TP):
            part = jnp.dot(hidden[:, block * FF_DEV:(block + 1) * FF_DEV], down_weight[expert][block * FF_DEV:(block + 1) * FF_DEV, :], preferred_element_type=jnp.float32)
            part = lax.optimization_barrier(part.astype(jnp.bfloat16))
            result = result + part.astype(jnp.float32)
        total = total.at[token_of].add(result * flat_shares[chosen][:, None])
        return (total, None)
    total, _ = lax.scan(one_expert, jnp.zeros((count_tok + 1, D), jnp.float32), jnp.arange(EXPERTS).astype(jnp.int32))
    expert_mix = total[:count_tok].astype(jnp.bfloat16)
    return (mixed_tokens, expert_mix)
```

```python
import jax
import jax.numpy as jnp
from jax import lax
from jax.sharding import PartitionSpec as P

WINDOW_MAX = 16


def from_everyone(value, axis):
    devices = lax.axis_size(axis)
    return lax.all_to_all(
        jnp.broadcast_to(value[None], (devices, *value.shape)), axis, 0, 0, tiled=True
    )


def joined_along(tiles, dim):
    tiles = jnp.moveaxis(tiles, 0, dim)
    shape = tiles.shape
    return tiles.reshape(*shape[:dim], shape[dim] * shape[dim + 1], *shape[dim + 2 :])


def collect(value, axis, dim):
    tiles = from_everyone(value, axis)
    return joined_along(tiles, dim)


def shifted(value, axis, by):
    devices = lax.axis_size(axis)
    pairs = [(i, i + by) for i in range(devices) if 0 <= i + by < devices]
    return lax.ppermute(value, axis, pairs)


def cut_along(value, dim, devices):
    shape = value.shape
    tiles = value.reshape(*shape[:dim], devices, shape[dim] // devices, *shape[dim + 1 :])
    return jnp.moveaxis(tiles, dim, 0)


def sent_and_summed(value, axis, dim):
    tiles = cut_along(value, dim, lax.axis_size(axis))
    arrived = lax.all_to_all(tiles, axis, split_axis=0, concat_axis=0, tiled=True)
    return arrived.astype(jnp.float32).sum(axis=0)


def exchange_in_groups(value, axis, split_dim, concat_dim, work, item_dim, out_dim):

    def moved(group):
        return lax.all_to_all(group, axis, split_axis=split_dim, concat_axis=concat_dim, tiled=True)

    items = jax.tree.leaves(value)[0].shape[item_dim]
    ends = [items * k // 2 for k in range(2 + 1)] if items % 2 == 0 else [0, items]
    groups = [
        jax.tree.map(lambda a: lax.slice_in_dim(a, low, high, axis=item_dim), value)
        for low, high in zip(ends, ends[1:])
    ]
    arrived = [moved(group) for group in groups]
    made = [work(group) for group in arrived]
    return jax.tree.map(lambda *parts: jnp.concatenate(parts, axis=out_dim), *made)


def rms_rows(rows, gain):
    values = rows.astype(jnp.float32)
    scaled = values * lax.rsqrt(jnp.mean(values * values, axis=-1, keepdims=True) + 1e-06)
    return (scaled * gain.astype(jnp.float32)).astype(jnp.bfloat16)


def expert_hidden(rows, w_gate, w_up):
    gate = jnp.dot(rows, w_gate, preferred_element_type=jnp.float32)
    upper = jnp.dot(rows, w_up, preferred_element_type=jnp.float32)
    return (jax.nn.silu(gate) * upper).astype(jnp.bfloat16)


def local(
    mixer_tokens,
    mixer_gain,
    in_weight,
    group_weight,
    channel_scale,
    out_weight,
    expert_tokens,
    expert_gain,
    route_ids,
    route_weights,
    gate_weight,
    up_weight,
    down_weight,
):
    normed = rms_rows(mixer_tokens, mixer_gain)
    pooled_in = jnp.dot(
        collect(normed, "tp", 0), in_weight, preferred_element_type=jnp.float32
    ).astype(jnp.bfloat16)
    block_rows = pooled_in.shape[0]
    rim_rows = shifted(pooled_in[block_rows - WINDOW_MAX :], "ep", 1)
    values = pooled_in.astype(jnp.float32)
    extended = jnp.concatenate([rim_rows.astype(jnp.float32), values], axis=0)
    window = jnp.left_shift(jnp.int32(2), lax.axis_index("tp"))
    sums = extended
    span = 1
    total = jnp.zeros_like(values)
    for level in range(WINDOW_MAX.bit_length() - 1):
        sums = sums[span:] + sums[:-span]
        span = span * 2
        total = total + jnp.where(window == span, sums[sums.shape[0] - block_rows :], 0.0)
    positions = lax.axis_index("ep") * block_rows + lax.iota(jnp.int32, block_rows) + 1
    counts = jnp.minimum(positions, window).astype(jnp.float32)
    pooled = (total / counts[:, None] - values).astype(jnp.bfloat16)
    grouped = (
        jnp.dot(pooled, group_weight[0], preferred_element_type=jnp.float32)
        * channel_scale.astype(jnp.float32)
    ).astype(jnp.bfloat16)
    rows = grouped
    mixed_tokens = sent_and_summed(
        jnp.dot(rows, out_weight, preferred_element_type=jnp.float32).astype(jnp.bfloat16), "tp", 0
    ).astype(jnp.bfloat16)
    expert_in = rms_rows(expert_tokens, expert_gain)
    shares = route_weights / jnp.sum(route_weights, axis=1, keepdims=True)
    rows_here, top_k = route_ids.shape
    width = expert_in.shape[1]
    n_experts = lax.axis_size("ep") * gate_weight.shape[0]
    capacity = 4 * rows_here // n_experts
    flat_ids = route_ids.reshape(rows_here * top_k)
    one_hot = (flat_ids[:, None] == jnp.arange(n_experts, dtype=jnp.int32)[None, :]).astype(
        jnp.int32
    )
    before = jnp.cumsum(one_hot, axis=0) - one_hot
    slots = jnp.sum(before * one_hot, axis=1)
    targets = flat_ids * capacity + slots
    placement = (
        targets.reshape(rows_here, top_k)[None, :, :]
        == jnp.arange(n_experts * capacity, dtype=jnp.int32)[:, None, None]
    )
    dispatch = jnp.any(placement, axis=2).astype(jnp.bfloat16)
    outgoing = jnp.dot(dispatch, expert_in, preferred_element_type=jnp.float32).astype(jnp.bfloat16)
    outgoing = outgoing.reshape(n_experts, capacity, width)

    gates = lax.all_gather(gate_weight[0], "tp", axis=0)
    uppers = lax.all_gather(up_weight[0], "tp", axis=0)
    downs = lax.all_gather(down_weight[0], "tp", axis=0)
    arrived = lax.all_to_all(outgoing, "ep", 0, 0, tiled=True).reshape(n_experts * capacity, width)
    made = jnp.zeros(arrived.shape, jnp.float32)
    for block in range(gates.shape[0]):
        hidden = expert_hidden(arrived, gates[block], uppers[block])
        made = made + jnp.dot(hidden, downs[block], preferred_element_type=jnp.float32)
    made = made.astype(jnp.bfloat16).reshape(n_experts, capacity, width)
    expert_out = lax.all_to_all(made, "ep", 0, 0, tiled=True).astype(jnp.float32)
    flat_out = expert_out.reshape(n_experts * capacity, width)
    picked = jnp.take(flat_out, targets, axis=0).reshape(rows_here, top_k, width)
    expert_mix = jnp.sum(picked * shares[:, :, None], axis=1).astype(jnp.bfloat16)
    return (mixed_tokens, expert_mix)


def solution(mesh):
    placed = (
        P(("grp", "ep", "tp"), None),
        P(),
        P(None, "tp"),
        P("tp", None, None),
        P("tp"),
        P("tp", None),
        P(("grp", "ep", "tp"), None),
        P(),
        P(("grp", "ep", "tp"), None),
        P(("grp", "ep", "tp"), None),
        P("ep", None, "tp"),
        P("ep", None, "tp"),
        P("ep", "tp", None),
    )
    return jax.shard_map(
        local,
        mesh=mesh,
        in_specs=placed,
        out_specs=(P(("grp", "ep", "tp"), None), P(("grp", "ep", "tp"), None)),
        check_vma=False,
    )
```

```python
import functools

import jax
import jax.numpy as jnp
from jax import lax
from jax.experimental import pallas as pl
from jax.experimental.pallas import tpu as pltpu
from jax.sharding import PartitionSpec as P

WINDOW_MAX = 16
META = 8
F32 = jnp.float32
BF16 = jnp.bfloat16


def from_everyone(value, axis):
    devices = lax.axis_size(axis)
    return lax.all_to_all(
        jnp.broadcast_to(value[None], (devices, *value.shape)), axis, 0, 0, tiled=True
    )


def shifted(value, axis, by):
    devices = lax.axis_size(axis)
    pairs = [(i, i + by) for i in range(devices) if 0 <= i + by < devices]
    return lax.ppermute(value, axis, pairs)


def rotated(value, axis, by):
    devices = lax.axis_size(axis)
    return lax.ppermute(value, axis, [(i, (i + by) % devices) for i in range(devices)])


def swapped(value, axis):
    devices = lax.axis_size(axis)
    return lax.ppermute(value, axis, [(i, i ^ 1) for i in range(devices)])


def rms_rows(rows, gain):
    values = rows.astype(F32)
    scaled = values * lax.rsqrt(jnp.mean(values * values, axis=-1, keepdims=True) + 1e-06)
    return (scaled * gain.astype(F32)).astype(BF16)


def call(body, outs, *operands, scalars=1, scratch=()):
    specs = [pl.BlockSpec(memory_space=pltpu.SMEM)] * scalars + [
        pl.BlockSpec(memory_space=pltpu.VMEM)
    ] * (len(operands) - scalars)
    return pl.pallas_call(
        body,
        out_shape=outs,
        in_specs=specs,
        out_specs=jax.tree.map(lambda _: pl.BlockSpec(memory_space=pltpu.VMEM), outs),
        scratch_shapes=list(scratch),
        compiler_params=pltpu.CompilerParams(vmem_limit_bytes=48 * 1024 * 1024),
    )(*operands)


def array(rows, width, dtype=BF16):
    return jax.ShapeDtypeStruct((rows, width), dtype)


def pack_body(ids_ref, weights_ref, tokens_ref, gain_ref, out_ref):
    rows, width = tokens_ref.shape
    values = tokens_ref[...].astype(F32)
    scaled = values * lax.rsqrt(jnp.mean(values * values, axis=-1, keepdims=True) + 1e-06)
    out_ref[0:rows, :] = (scaled * gain_ref[...].astype(F32)).astype(BF16)
    weights = weights_ref[...]
    first, second = weights[0:1], weights[1:2]
    both = first + second
    lines = [ids_ref[0:1].astype(F32), ids_ref[1:2].astype(F32)]
    for share in (first / both, second / both):
        high = share.astype(BF16).astype(F32)
        lines += [high, share - high]
    lines += [jnp.zeros_like(first)] * (META - len(lines))
    meta = jnp.concatenate(lines, axis=0)
    meta = jnp.concatenate([meta, jnp.zeros((META, width - rows), F32)], axis=1)
    out_ref[rows:, :] = meta.astype(BF16)


def slots_of(block_ref, place_ref, chips, sign, count, capacity, kept):
    rows = block_ref.shape[0] - META
    meta = block_ref[rows:, 0:rows].astype(F32)
    chip, core = place_ref[0], place_ref[1]
    index = lax.broadcasted_iota(jnp.int32, (count, rows), 0)
    step = lax.shift_right_logical(index, 1)
    first = 1 if sign else 0
    named = chip + sign * (first + step) + chips
    named = jnp.where(named >= chips, named - chips, named)
    named = jnp.where(named >= chips, named - chips, named)
    expert = (2 * named + ((core + (index & 1)) & 1)).astype(F32)
    is_first, is_second = meta[0:1] == expert, meta[1:2] == expert
    match = jnp.where(is_first, 1.0, 0.0) + jnp.where(is_second, 1.0, 0.0)
    shares = jnp.where(is_first, meta[2:3] + meta[3:4], 0.0) + jnp.where(
        is_second, meta[4:5] + meta[5:6], 0.0
    )
    upto = (
        lax.broadcasted_iota(jnp.int32, (rows, rows), 0)
        <= lax.broadcasted_iota(jnp.int32, (rows, rows), 1)
    ).astype(F32).astype(BF16)
    rank = jnp.dot(match.astype(BF16), upto, preferred_element_type=F32)
    slot = jnp.where(match > 0.5, rank - 1.0, -1.0)
    number = lax.broadcasted_iota(jnp.int32, (capacity, rows), 0).astype(F32)
    hot = [jnp.where(slot[e : e + 1] == number, 1.0, 0.0) for e in kept]
    return hot, [shares[e : e + 1] for e in kept]


def picked(hot, block_ref):
    rows = block_ref.shape[0] - META
    chosen = jnp.concatenate(hot, axis=0).astype(BF16)
    return jnp.dot(chosen, block_ref[0:rows, :], preferred_element_type=F32).astype(BF16)


def spread(hot, shares, results):
    scaled = [
        (jnp.sum(h * s, axis=1, keepdims=True) * r.astype(F32)).astype(BF16)
        for h, s, r in zip(hot, shares, results)
    ]
    return lax.dot_general(
        jnp.concatenate(hot, axis=0).astype(BF16),
        jnp.concatenate(scaled, axis=0),
        (((0,), (0,)), ((), ())),
        preferred_element_type=F32,
    )


KEPT = {1: (0, 1, 2, 3, 4, 5, 6), -1: (0, 1, 2, 3, 4, 5, 7)}


def far_cuts(capacity):
    return [(2 * capacity * k, 2 * capacity * k + 2 * capacity) for k in range(3)] + [
        (6 * capacity, 7 * capacity)
    ]


def relay_body(chips, capacity, place_ref, up_ref, down_ref, *outs):
    for sign, block_ref, own in ((1, up_ref, outs[:4]), (-1, down_ref, outs[4:])):
        hot, _ = slots_of(block_ref, place_ref, chips, sign, 8, capacity, KEPT[sign])
        rows = picked(hot, block_ref)
        for (low, high), out_ref in zip(far_cuts(capacity), own):
            out_ref[...] = rows[low:high]


def near_body(chips, capacity, place_ref, *refs):
    blocks, (same_ref, other_ref) = refs[:-2], refs[-2:]
    for i, block_ref in enumerate(blocks):
        hot, _ = slots_of(block_ref, place_ref, chips, 0, 8, capacity, (0, 1))
        rows = picked(hot, block_ref)
        same_ref[i * capacity : (i + 1) * capacity, :] = rows[:capacity]
        other_ref[i * capacity : (i + 1) * capacity, :] = rows[capacity:]


def unpack_body(capacity, *refs):
    far, (same_ref, other_ref) = refs[:-2], refs[-2:]
    same = [far[i][0:capacity, :] for i in (0, 1, 2, 3, 4, 5, 6)]
    other = [far[i][capacity : 2 * capacity, :] for i in (0, 1, 2, 4, 5, 6)] + [far[7][...]]
    for i in range(7):
        same_ref[i * capacity : (i + 1) * capacity, :] = same[i]
        other_ref[i * capacity : (i + 1) * capacity, :] = other[i]


def hidden_body(parts, cuts, *refs):
    rows = jnp.concatenate([ref[...] for ref in refs[:parts]], axis=0)
    weights, out_ref, at = list(refs[parts:-1]), refs[-1], 0
    for pieces in cuts:
        values = []
        for _ in range(2):
            total, low = 0.0, 0
            for _ in range(pieces):
                ref = weights.pop(0)
                total = total + jnp.dot(
                    rows[:, low : low + ref.shape[0]], ref[...], preferred_element_type=F32
                )
                low += ref.shape[0]
            values.append(total)
        gate, upper = values
        made = gate / (1.0 + jnp.exp(-gate)) * upper
        out_ref[:, at : at + made.shape[1]] = made.astype(BF16)
        at += made.shape[1]


def down_body(sizes, count, *refs):
    hidden = jnp.concatenate([ref[...] for ref in refs[:count]], axis=1)
    outs = refs[len(refs) - len(sizes) :]
    total, low = 0.0, 0
    for ref in refs[count : len(refs) - len(sizes)]:
        total = total + jnp.dot(
            hidden[:, low : low + ref.shape[0]], ref[...], preferred_element_type=F32
        )
        low += ref.shape[0]
    at = 0
    for size, out_ref in zip(sizes, outs):
        out_ref[...] = total[at : at + size].astype(BF16)
        at += size


def far_back_body(capacity, same_ref, other_ref, *outs):
    for i in range(3):
        for base, own in ((0, outs[:4]), (4, outs[4:])):
            j = i + base
            k = i if base == 0 else i + 3
            own[i][0:capacity, :] = same_ref[j * capacity : (j + 1) * capacity, :]
            own[i][capacity:, :] = other_ref[k * capacity : (k + 1) * capacity, :]
    outs[3][...] = same_ref[3 * capacity : 4 * capacity, :]
    outs[7][...] = other_ref[6 * capacity : 7 * capacity, :]


def own_part(block_ref, place_ref, same_ref, other_ref, i, chips, capacity):
    hot, shares = slots_of(block_ref, place_ref, chips, 0, 8, capacity, (0, 1))
    low, high = i * capacity, (i + 1) * capacity
    return spread(hot, shares, [same_ref[low:high, :], other_ref[low:high, :]])


def turn_body(chips, capacity, at, place_ref, up_ref, down_ref, same_ref, other_ref, *refs):
    far, outs = refs[:8], refs[8:]
    for sign, block_ref, own, i, out_ref in (
        (1, up_ref, far[:4], at[0], outs[0]),
        (-1, down_ref, far[4:], at[1], outs[1]),
    ):
        hot, shares = slots_of(block_ref, place_ref, chips, sign, 8, capacity, KEPT[sign])
        results = []
        for ref in own:
            for low in range(0, ref.shape[0], capacity):
                results.append(ref[low : low + capacity, :])
        total = spread(hot, shares, results)
        total = total + own_part(block_ref, place_ref, same_ref, other_ref, i, chips, capacity)
        out_ref[...] = total.astype(BF16)


def near_back_body(chips, capacity, count, place_ref, *refs):
    blocks = refs[:count]
    same_ref, other_ref = refs[count : count + 2]
    for i, (block_ref, out_ref) in enumerate(zip(blocks, refs[count + 2 :])):
        total = own_part(block_ref, place_ref, same_ref, other_ref, i, chips, capacity)
        out_ref[...] = total.astype(BF16)


def summed(*values):
    total = values[0].astype(F32)
    for value in values[1:]:
        total = total + value.astype(F32)
    return total.astype(BF16)


def mixer(mixer_tokens, mixer_gain, in_weight, group_weight, channel_scale, out_weight):
    normed = rms_rows(mixer_tokens, mixer_gain)
    pooled_in = jnp.dot(
        from_everyone(normed, "tp").reshape(-1, normed.shape[1]),
        in_weight,
        preferred_element_type=F32,
    ).astype(BF16)
    block_rows = pooled_in.shape[0]
    rim_rows = shifted(pooled_in[block_rows - WINDOW_MAX :], "ep", 1)
    values = pooled_in.astype(F32)
    extended = jnp.concatenate([rim_rows.astype(F32), values], axis=0)
    window = jnp.left_shift(jnp.int32(2), lax.axis_index("tp"))
    sums = extended
    span = 1
    total = jnp.zeros_like(values)
    for _ in range(WINDOW_MAX.bit_length() - 1):
        sums = sums[span:] + sums[:-span]
        span = span * 2
        total = total + jnp.where(window == span, sums[sums.shape[0] - block_rows :], 0.0)
    positions = lax.axis_index("ep") * block_rows + lax.iota(jnp.int32, block_rows) + 1
    counts = jnp.minimum(positions, window).astype(F32)
    pooled = (total / counts[:, None] - values).astype(BF16)
    grouped = (
        jnp.dot(pooled, group_weight[0], preferred_element_type=F32) * channel_scale.astype(F32)
    ).astype(BF16)
    made = jnp.dot(grouped, out_weight, preferred_element_type=F32).astype(BF16)
    made = made.reshape(lax.axis_size("tp"), -1, made.shape[1])
    arrived = lax.all_to_all(made, "tp", split_axis=0, concat_axis=0, tiled=True)
    return arrived.astype(F32).sum(axis=0).astype(BF16)


def local(
    mixer_tokens,
    mixer_gain,
    in_weight,
    group_weight,
    channel_scale,
    out_weight,
    expert_tokens,
    expert_gain,
    route_ids,
    route_weights,
    gate_weight,
    up_weight,
    down_weight,
):
    rows, width = expert_tokens.shape
    chips = lax.axis_size("ep") // 2
    capacity = 4 * rows // (2 * chips)
    place = jnp.stack([lax.axis_index("ep") // 2, lax.axis_index("ep") % 2]).astype(jnp.int32)
    block_rows = rows + META

    own = [gate_weight[0], up_weight[0], down_weight[0]]
    from_left = [rotated(w, "tp", 1) for w in own]
    from_right = [rotated(w, "tp", -1) for w in own]
    opposite = [
        (
            rotated(left[: left.shape[0] // 2], "tp", 1),
            rotated(right[right.shape[0] // 2 :], "tp", -1),
        )
        for left, right in zip(from_left, from_right)
    ]

    block = call(
        pack_body,
        array(block_rows, width),
        route_ids.T,
        route_weights.T,
        expert_tokens,
        expert_gain[None],
        scalars=0,
    )
    ups, downs = [block], [block]
    for _ in range(4):
        ups.append(rotated(ups[-1], "ep", 2))
        downs.append(rotated(downs[-1], "ep", -2))
    pieces = [array(high - low, width) for low, high in far_cuts(capacity)]
    far = call(
        functools.partial(relay_body, chips, capacity), pieces * 2, place, ups[4], downs[4]
    )
    far = [rotated(far[k], "ep", 2 * (k + 1)) for k in range(4)] + [
        rotated(far[4 + k], "ep", -2 * (k + 1)) for k in range(4)
    ]
    blocks = [block] + ups[1:4] + downs[1:4] + [ups[4], downs[4]]
    near_same, near_other = call(
        functools.partial(near_body, chips, capacity),
        [array(9 * capacity, width)] * 2,
        place,
        *blocks,
    )
    near_other = swapped(near_other, "ep")
    far_same, far_other = call(
        functools.partial(unpack_body, capacity), [array(7 * capacity, width)] * 2, *far, scalars=0
    )
    far_other = swapped(far_other, "ep")

    parts = [near_same, far_same, near_other, far_other]
    total = sum(p.shape[0] for p in parts)
    ff = own[0].shape[1]
    hidden_near = call(
        functools.partial(hidden_body, 4, (1, 1, 1)),
        array(total, 3 * ff),
        *parts,
        own[0],
        own[1],
        from_left[0],
        from_left[1],
        from_right[0],
        from_right[1],
        scalars=0,
    )
    hidden_far = call(
        functools.partial(hidden_body, 4, (2,)),
        array(total, ff),
        *parts,
        *opposite[0],
        *opposite[1],
        scalars=0,
    )
    sizes = [p.shape[0] for p in parts]
    near_same, far_same, near_other, far_other = call(
        functools.partial(down_body, sizes, 2),
        [array(size, width) for size in sizes],
        hidden_near,
        hidden_far,
        own[2],
        from_left[2],
        from_right[2],
        *opposite[2],
        scalars=0,
    )

    far_other = swapped(far_other, "ep")
    near_other = swapped(near_other, "ep")
    back = call(
        functools.partial(far_back_body, capacity), pieces * 2, far_same, far_other, scalars=0
    )
    back = [rotated(back[k], "ep", -2 * (k + 1)) for k in range(4)] + [
        rotated(back[4 + k], "ep", 2 * (k + 1)) for k in range(4)
    ]
    kept = call(
        functools.partial(near_back_body, chips, capacity, 7),
        [array(rows, width)] * 7,
        place,
        *blocks[:7],
        near_same,
        near_other,
    )
    up_sum, down_sum = call(
        functools.partial(turn_body, chips, capacity, (7, 8)),
        [array(rows, width)] * 2,
        place,
        ups[4],
        downs[4],
        near_same,
        near_other,
        *back,
    )
    for k in (3, 2, 1):
        up_sum = summed(rotated(up_sum, "ep", -2), kept[k])
        down_sum = summed(rotated(down_sum, "ep", 2), kept[3 + k])
    expert_mix = summed(rotated(up_sum, "ep", -2), rotated(down_sum, "ep", 2), kept[0])

    mixed_tokens = mixer(
        mixer_tokens, mixer_gain, in_weight, group_weight, channel_scale, out_weight
    )
    return (mixed_tokens, expert_mix)


def solution(mesh):
    placed = (
        P(("grp", "ep", "tp"), None),
        P(),
        P(None, "tp"),
        P("tp", None, None),
        P("tp"),
        P("tp", None),
        P(("grp", "ep", "tp"), None),
        P(),
        P(("grp", "ep", "tp"), None),
        P(("grp", "ep", "tp"), None),
        P("ep", None, "tp"),
        P("ep", None, "tp"),
        P("ep", "tp", None),
    )
    return jax.shard_map(
        local,
        mesh=mesh,
        in_specs=placed,
        out_specs=(P(("grp", "ep", "tp"), None), P(("grp", "ep", "tp"), None)),
        check_vma=False,
    )
```

```python
import functools

import jax
import jax.numpy as jnp
from jax import lax
from jax.experimental import pallas as pl
from jax.experimental.pallas import tpu as pltpu
from jax.sharding import PartitionSpec as P


WINDOW_MAX = 16
META = 8
F32 = jnp.float32
BF16 = jnp.bfloat16


def shifted(value, axis, by):
    devices = lax.axis_size(axis)
    pairs = [(i, i + by) for i in range(devices) if 0 <= i + by < devices]
    return lax.ppermute(value, axis, pairs)


def rotated(value, axis, by):
    devices = lax.axis_size(axis)
    return lax.ppermute(value, axis, [(i, (i + by) % devices) for i in range(devices)])


def stepped(value, by):
    sides, members = lax.axis_size("ep"), lax.axis_size("tp")
    pairs = []
    for i in range(sides):
        step = by if i % 2 == 0 else -by
        pairs += [(i * members + j, i * members + (j + step) % members) for j in range(members)]
    return lax.ppermute(value, ("ep", "tp"), pairs)


def swapped(value, axis):
    devices = lax.axis_size(axis)
    return lax.ppermute(value, axis, [(i, i ^ 1) for i in range(devices)])


def call(mib, body, outs, *operands, scalars=1, waits=0, scratch=()):
    specs = (
        [pl.BlockSpec(memory_space=pltpu.SMEM)] * scalars
        + [pl.BlockSpec(memory_space=pltpu.VMEM)] * (len(operands) - scalars - waits)
        + [pl.BlockSpec(memory_space=pl.ANY)] * waits
    )
    return pl.pallas_call(
        body,
        out_shape=outs,
        in_specs=specs,
        out_specs=jax.tree.map(lambda _: pl.BlockSpec(memory_space=pltpu.VMEM), outs),
        scratch_shapes=list(scratch),
        compiler_params=pltpu.CompilerParams(vmem_limit_bytes=mib * 1024 * 1024),
    )(*operands)


def array(rows, width, dtype=BF16):
    return jax.ShapeDtypeStruct((rows, width), dtype)


def pack_body(ids_ref, weights_ref, tokens_ref, gain_ref, out_ref):
    rows, width = tokens_ref.shape
    values = tokens_ref[...].astype(F32)
    scaled = values * lax.rsqrt(jnp.mean(values * values, axis=-1, keepdims=True) + 1e-06)
    out_ref[0:rows, :] = (scaled * gain_ref[...].astype(F32)).astype(BF16)
    weights = weights_ref[...]
    first, second = weights[0:1], weights[1:2]
    both = first + second
    lines = [ids_ref[0:1].astype(F32), ids_ref[1:2].astype(F32)]
    for share in (first / both, second / both):
        high = share.astype(BF16).astype(F32)
        lines += [high, share - high]
    lines += [jnp.zeros_like(first)] * (META - len(lines))
    meta = jnp.concatenate(lines, axis=0)
    meta = jnp.concatenate([meta, jnp.zeros((META, width - rows), F32)], axis=1)
    out_ref[rows:, :] = meta.astype(BF16)


def slots_of(block_ref, place_ref, chips, sign, count, capacity, kept):
    rows = block_ref.shape[0] - META
    meta = block_ref[rows:, 0:rows].astype(F32)
    chip, core = place_ref[0], place_ref[1]
    index = lax.broadcasted_iota(jnp.int32, (count, rows), 0)
    step = lax.shift_right_logical(index, 1)
    first = 1 if sign else 0
    named = chip + sign * (first + step) + chips
    named = jnp.where(named >= chips, named - chips, named)
    named = jnp.where(named >= chips, named - chips, named)
    expert = (2 * named + ((core + (index & 1)) & 1)).astype(F32)
    is_first, is_second = meta[0:1] == expert, meta[1:2] == expert
    match = jnp.where(is_first, 1.0, 0.0) + jnp.where(is_second, 1.0, 0.0)
    shares = jnp.where(is_first, meta[2:3] + meta[3:4], 0.0) + jnp.where(
        is_second, meta[4:5] + meta[5:6], 0.0
    )
    upto = (
        lax.broadcasted_iota(jnp.int32, (rows, rows), 0)
        <= lax.broadcasted_iota(jnp.int32, (rows, rows), 1)
    ).astype(F32).astype(BF16)
    rank = jnp.dot(match.astype(BF16), upto, preferred_element_type=F32)
    slot = jnp.where(match > 0.5, rank - 1.0, -1.0)
    number = lax.broadcasted_iota(jnp.int32, (capacity, rows), 0).astype(F32)
    hot = [jnp.where(slot[e : e + 1] == number, 1.0, 0.0) for e in kept]
    return hot, [shares[e : e + 1] for e in kept]


def by_columns(width, body, pieces=4):
    @pl.loop(0, pieces)
    def _(i):
        body(pl.ds(pl.multiple_of(i * (width // pieces), 128), width // pieces))


def picked(chosen, block_ref, columns):
    rows = block_ref.shape[0] - META
    return jnp.dot(chosen, block_ref[0:rows, columns], preferred_element_type=F32).astype(BF16)


def weighed(hot, shares):
    values = [jnp.sum(h * s, axis=1, keepdims=True) for h, s in zip(hot, shares)]
    return jnp.concatenate(hot, axis=0).T.astype(BF16), values


def spread(chosen, values, results):
    scaled = [(v * r.astype(F32)).astype(BF16) for v, r in zip(values, results)]
    return jnp.dot(chosen, jnp.concatenate(scaled, axis=0), preferred_element_type=F32)


KEPT = {1: (0, 1, 2, 3, 4, 5, 6), -1: (0, 1, 2, 3, 4, 5, 7)}


def far_cuts(capacity):
    return [(2 * capacity * k, 2 * capacity * k + 2 * capacity) for k in range(3)] + [
        (6 * capacity, 7 * capacity)
    ]


def relay_body(chips, capacity, place_ref, up_ref, down_ref, *outs):
    todo = []
    for sign, block_ref, own in ((1, up_ref, outs[:4]), (-1, down_ref, outs[4:])):
        hot, _ = slots_of(block_ref, place_ref, chips, sign, 8, capacity, KEPT[sign])
        todo.append((jnp.concatenate(hot, axis=0).astype(BF16), block_ref, own))

    def piece(columns):
        for chosen, block_ref, own in todo:
            rows = picked(chosen, block_ref, columns)
            for (low, high), out_ref in zip(far_cuts(capacity), own):
                out_ref[:, columns] = rows[low:high]

    by_columns(up_ref.shape[1], piece)


def near_body(chips, capacity, place_ref, *refs):
    blocks, (same_ref, other_ref) = refs[:-2], refs[-2:]
    chosen = []
    for block_ref in blocks:
        hot, _ = slots_of(block_ref, place_ref, chips, 0, 8, capacity, (0, 1))
        chosen.append(jnp.concatenate(hot, axis=0).astype(BF16))

    def piece(columns):
        for i, block_ref in enumerate(blocks):
            rows = picked(chosen[i], block_ref, columns)
            same_ref[i * capacity : (i + 1) * capacity, columns] = rows[:capacity]
            other_ref[i * capacity : (i + 1) * capacity, columns] = rows[capacity:]

    by_columns(same_ref.shape[1], piece)


def unpack_body(capacity, *refs):
    far, (same_ref, other_ref) = refs[:-2], refs[-2:]
    same = [far[i][0:capacity, :] for i in (0, 1, 2, 3, 4, 5, 6)]
    other = [far[i][capacity : 2 * capacity, :] for i in (0, 1, 2, 4, 5, 6)] + [far[7][...]]
    for i in range(7):
        same_ref[i * capacity : (i + 1) * capacity, :] = same[i]
        other_ref[i * capacity : (i + 1) * capacity, :] = other[i]


def hidden_body(count, pairs, *refs):
    parts, weights, out_ref, rows_ref = refs[:count], refs[count : count + 2 * pairs], refs[-2], refs[-1]
    low = 0
    for ref in parts:
        rows_ref[low : low + ref.shape[0], :] = ref[...]
        low += ref.shape[0]

    @pl.loop(0, 2)
    def _(i):
        here = pl.ds(pl.multiple_of(i * (low // 2), 128), low // 2)
        for k in range(pairs):
            gate = jnp.dot(rows_ref[here, :], weights[2 * k][...], preferred_element_type=F32)
            upper = jnp.dot(rows_ref[here, :], weights[2 * k + 1][...], preferred_element_type=F32)
            made = (gate / (1.0 + jnp.exp(-gate)) * upper).astype(BF16)
            columns = made.shape[1]
            out_ref[here, k * columns : (k + 1) * columns] = made


def down_body(first, sizes, count, *refs):
    rows = sum(sizes)
    hidden = jnp.concatenate([ref[first : first + rows, :] for ref in refs[:count]], axis=1)
    outs = refs[len(refs) - len(sizes) :]
    weights = refs[count : len(refs) - len(sizes)]

    def piece(columns):
        total, low = 0.0, 0
        for ref in weights:
            total = total + jnp.dot(
                hidden[:, low : low + ref.shape[0]], ref[:, columns], preferred_element_type=F32
            )
            low += ref.shape[0]
        at = 0
        for size, out_ref in zip(sizes, outs):
            out_ref[:, columns] = total[at : at + size].astype(BF16)
            at += size

    by_columns(outs[0].shape[1], piece)


def far_back_body(capacity, same_ref, other_ref, *outs):
    for i in range(3):
        for base, own in ((0, outs[:4]), (4, outs[4:])):
            j = i + base
            k = i if base == 0 else i + 3
            own[i][0:capacity, :] = same_ref[j * capacity : (j + 1) * capacity, :]
            own[i][capacity:, :] = other_ref[k * capacity : (k + 1) * capacity, :]
    outs[3][...] = same_ref[3 * capacity : 4 * capacity, :]
    outs[7][...] = other_ref[6 * capacity : 7 * capacity, :]


def own_weighed(block_ref, place_ref, chips, capacity):
    return weighed(*slots_of(block_ref, place_ref, chips, 0, 8, capacity, (0, 1)))


def own_part(made, i, capacity, same_ref, other_ref, columns):
    low, high = i * capacity, (i + 1) * capacity
    return spread(*made, [same_ref[low:high, columns], other_ref[low:high, columns]])


def turn_body(chips, capacity, at, place_ref, up_ref, down_ref, same_ref, other_ref, *refs):
    far, outs = refs[:8], refs[8:]
    todo = []
    for sign, block_ref, own, i, out_ref in (
        (1, up_ref, far[:4], at[0], outs[0]),
        (-1, down_ref, far[4:], at[1], outs[1]),
    ):
        made = weighed(*slots_of(block_ref, place_ref, chips, sign, 8, capacity, KEPT[sign]))
        near = own_weighed(block_ref, place_ref, chips, capacity)
        todo.append((made, near, own, i, out_ref))

    def piece(columns):
        for made, near, own, i, out_ref in todo:
            results = []
            for ref in own:
                for low in range(0, ref.shape[0], capacity):
                    results.append(ref[low : low + capacity, columns])
            total = spread(*made, results)
            total = total + own_part(near, i, capacity, same_ref, other_ref, columns)
            out_ref[:, columns] = total.astype(BF16)

    by_columns(up_ref.shape[1], piece)


def near_back_body(chips, capacity, count, place_ref, *refs):
    blocks = refs[:count]
    same_ref, other_ref = refs[count : count + 2]
    outs = refs[count + 2 :]
    near = [own_weighed(block_ref, place_ref, chips, capacity) for block_ref in blocks]

    def piece(columns):
        for i, out_ref in enumerate(outs):
            total = own_part(near[i], i, capacity, same_ref, other_ref, columns)
            out_ref[:, columns] = total.astype(BF16)

    by_columns(same_ref.shape[1], piece)


def mixer_norm_body(tokens_ref, gain_ref, _, out_ref):
    values = tokens_ref[...].astype(F32)
    scaled = values * lax.rsqrt(jnp.mean(values * values, axis=-1, keepdims=True) + 1e-06)
    out_ref[...] = (scaled * gain_ref[...].astype(F32)).astype(BF16)


def mixer_first_body(members, place_ref, *refs):
    blocks, weight_ref, out_ref = refs[:members], refs[members], refs[members + 1]
    rows = blocks[0].shape[0]
    for k, block_ref in enumerate(blocks):
        at = lax.rem(place_ref[2] + k, members) * rows
        made = jnp.dot(block_ref[...], weight_ref[...], preferred_element_type=F32)
        out_ref[pl.ds(pl.multiple_of(at, rows), rows), :] = made.astype(BF16)


def mixer_second_body(members, place_ref, rim_ref, rows_ref, group_ref, scale_ref, weight_ref, *refs):
    outs, extended_ref = refs[:members], refs[members]
    rim, total = rim_ref.shape[0], rows_ref.shape[0]
    rows = total // members
    extended_ref[0:rim, :] = rim_ref[...]
    extended_ref[rim:, :] = rows_ref[...]
    window = lax.shift_left(jnp.int32(2), place_ref[2])
    behind = (
        lax.broadcasted_iota(jnp.int32, (rows, rows + rim), 0)
        - lax.broadcasted_iota(jnp.int32, (rows, rows + rim), 1)
        + rim
    )
    inside = jnp.where((behind >= 0) & (behind < window), 1.0, 0.0).astype(BF16)
    grouped = []
    for k in range(members):
        at = pl.multiple_of(lax.rem(place_ref[2] + k, members) * rows, rows)
        values = rows_ref[pl.ds(at, rows), :].astype(F32)
        sums = jnp.dot(
            inside, extended_ref[pl.ds(at, rows + rim), :], preferred_element_type=F32
        )
        position = place_ref[3] * total + at + 1 + lax.broadcasted_iota(jnp.int32, (rows, 1), 0)
        counts = jnp.minimum(position, window).astype(F32)
        pooled = (sums / counts - values).astype(BF16)
        made = jnp.dot(pooled, group_ref[...], preferred_element_type=F32)
        grouped.append((made * scale_ref[...].astype(F32)).astype(BF16))
    grouped = jnp.concatenate(grouped, axis=0)

    def piece(columns):
        made = jnp.dot(grouped, weight_ref[:, columns], preferred_element_type=F32).astype(BF16)
        for k, out_ref in enumerate(outs):
            out_ref[:, columns] = made[k * rows : (k + 1) * rows]

    by_columns(weight_ref.shape[1], piece)


def summed(*values):
    total = values[0].astype(F32)
    for value in values[1:]:
        total = total + value.astype(F32)
    return total.astype(BF16)


def mixer(
    place, mixer_tokens, mixer_gain, in_weight, group_weight, channel_scale, out_weight, wait
):
    rows, width = mixer_tokens.shape
    members = lax.axis_size("tp")
    columns = in_weight.shape[1]
    normed = call(
        6,
        mixer_norm_body,
        array(rows, width),
        mixer_tokens,
        mixer_gain[None],
        wait,
        scalars=0,
        waits=1,
    )
    blocks = [normed] + [rotated(normed, "tp", -k) for k in range(1, members)]
    pooled_in = call(
        12,
        functools.partial(mixer_first_body, members),
        array(rows * members, columns),
        place,
        *blocks,
        in_weight,
    )
    rim = shifted(pooled_in[rows * members - WINDOW_MAX :], "ep", 1)
    parts = call(
        16,
        functools.partial(mixer_second_body, members),
        [array(rows, width)] * members,
        place,
        rim,
        pooled_in,
        group_weight[0],
        channel_scale[None],
        out_weight,
        scratch=[pltpu.VMEM((rows * members + WINDOW_MAX, columns), BF16)],
    )
    parts = [parts[0]] + [rotated(parts[k], "tp", k) for k in range(1, members)]
    return summed(*parts)


def local(
    mixer_tokens,
    mixer_gain,
    in_weight,
    group_weight,
    channel_scale,
    out_weight,
    expert_tokens,
    expert_gain,
    route_ids,
    route_weights,
    gate_weight,
    up_weight,
    down_weight,
):
    rows, width = expert_tokens.shape
    chips = lax.axis_size("ep") // 2
    capacity = 4 * rows // (2 * chips)
    side = lax.axis_index("ep")
    place = jnp.stack([side // 2, side % 2, lax.axis_index("tp"), side]).astype(jnp.int32)
    block_rows = rows + META

    own = [gate_weight[0], up_weight[0], down_weight[0]]
    one = [(stepped(w, 1), stepped(w, -1)) for w in own]
    two = [stepped(pair[0], 1) for pair in one[:2]]
    two.append(stepped(one[2][0], 1))

    block = call(
        6,
        pack_body,
        array(block_rows, width),
        route_ids.T,
        route_weights.T,
        expert_tokens,
        expert_gain[None],
        scalars=0,
    )
    ups, downs = [block], [block]
    for _ in range(4):
        ups.append(rotated(ups[-1], "ep", 2))
        downs.append(rotated(downs[-1], "ep", -2))
    pieces = [array(high - low, width) for low, high in far_cuts(capacity)]
    far = call(
        8, functools.partial(relay_body, chips, capacity), pieces * 2, place, ups[4], downs[4]
    )
    far = [rotated(far[k], "ep", 2 * (k + 1)) for k in range(4)] + [
        rotated(far[4 + k], "ep", -2 * (k + 1)) for k in range(4)
    ]
    blocks = [block] + ups[1:4] + downs[1:4] + [ups[4], downs[4]]
    near_same, near_other = call(
        12,
        functools.partial(near_body, chips, capacity),
        [array(9 * capacity, width)] * 2,
        place,
        *blocks,
    )
    near_other = swapped(near_other, "ep")
    far_same, far_other = call(
        6,
        functools.partial(unpack_body, capacity),
        [array(7 * capacity, width)] * 2,
        *far,
        scalars=0,
    )
    far_other = swapped(far_other, "ep")

    parts = [far_same, far_other, near_same, near_other]
    sizes = [p.shape[0] for p in parts]
    total = sum(sizes)
    ff = own[0].shape[1]
    rows_scratch = [pltpu.VMEM((total, width), BF16)]
    hidden = call(
        24,
        functools.partial(hidden_body, 4, 3),
        array(total, 3 * ff),
        *parts,
        own[0],
        own[1],
        one[0][0],
        one[1][0],
        one[0][1],
        one[1][1],
        scalars=0,
        scratch=rows_scratch,
    )
    hidden_last = call(
        16,
        functools.partial(hidden_body, 4, 1),
        array(total, ff),
        *parts,
        two[0],
        two[1],
        hidden,
        scalars=0,
        waits=1,
        scratch=rows_scratch,
    )

    def results(first, sizes):
        return call(
            16,
            functools.partial(down_body, first, sizes, 2),
            [array(size, width) for size in sizes],
            hidden,
            hidden_last,
            own[2],
            *one[2],
            two[2],
            scalars=0,
        )

    far_same, far_other = results(0, sizes[:2])
    near_same, near_other = results(sum(sizes[:2]), sizes[2:])

    far_other = swapped(far_other, "ep")
    near_other = swapped(near_other, "ep")
    back = call(
        6, functools.partial(far_back_body, capacity), pieces * 2, far_same, far_other, scalars=0
    )
    back = [rotated(back[k], "ep", -2 * (k + 1)) for k in range(4)] + [
        rotated(back[4 + k], "ep", 2 * (k + 1)) for k in range(4)
    ]
    kept = call(
        16,
        functools.partial(near_back_body, chips, capacity, 7),
        [array(rows, width)] * 7,
        place,
        *blocks[:7],
        near_same,
        near_other,
    )
    up_sum, down_sum = call(
        10,
        functools.partial(turn_body, chips, capacity, (7, 8)),
        [array(rows, width)] * 2,
        place,
        ups[4],
        downs[4],
        near_same,
        near_other,
        *back,
    )
    for k in (3, 2, 1, 0):
        up_sum = rotated(up_sum, "ep", -2)
        down_sum = rotated(down_sum, "ep", 2)
        if k > 0:
            up_sum = summed(up_sum, kept[k])
            down_sum = summed(down_sum, kept[3 + k])
    expert_mix = summed(up_sum, down_sum, kept[0])

    mixed_tokens = mixer(
        place,
        mixer_tokens,
        mixer_gain,
        in_weight,
        group_weight,
        channel_scale,
        out_weight,
        hidden_last,
    )
    return (mixed_tokens, expert_mix)


def solution(mesh):
    placed = (
        P(("grp", "ep", "tp"), None),
        P(),
        P(None, "tp"),
        P("tp", None, None),
        P("tp"),
        P("tp", None),
        P(("grp", "ep", "tp"), None),
        P(),
        P(("grp", "ep", "tp"), None),
        P(("grp", "ep", "tp"), None),
        P("ep", None, "tp"),
        P("ep", None, "tp"),
        P("ep", "tp", None),
    )

    return jax.shard_map(
        local,
        mesh=mesh,
        in_specs=placed,
        out_specs=(P(("grp", "ep", "tp"), None), P(("grp", "ep", "tp"), None)),
        check_vma=False,
    )
```

```python
import functools

import jax
import jax.numpy as jnp
from jax import lax
from jax.experimental import pallas as pl
from jax.experimental.pallas import tpu as pltpu
from jax.sharding import PartitionSpec as P


WINDOW_MAX = 16
META = 8
F32 = jnp.float32
BF16 = jnp.bfloat16


def shifted(value, axis, by):
    devices = lax.axis_size(axis)
    pairs = [(i, i + by) for i in range(devices) if 0 <= i + by < devices]
    return lax.ppermute(value, axis, pairs)


def rotated(value, axis, by):
    devices = lax.axis_size(axis)
    return lax.ppermute(value, axis, [(i, (i + by) % devices) for i in range(devices)])


def swapped(value, axis):
    devices = lax.axis_size(axis)
    return lax.ppermute(value, axis, [(i, i ^ 1) for i in range(devices)])


def call(mib, body, outs, *operands, scalars=1, waits=0, scratch=()):
    specs = (
        [pl.BlockSpec(memory_space=pltpu.SMEM)] * scalars
        + [pl.BlockSpec(memory_space=pltpu.VMEM)] * (len(operands) - scalars - waits)
        + [pl.BlockSpec(memory_space=pl.ANY)] * waits
    )
    return pl.pallas_call(
        body,
        out_shape=outs,
        in_specs=specs,
        out_specs=jax.tree.map(lambda _: pl.BlockSpec(memory_space=pltpu.VMEM), outs),
        scratch_shapes=list(scratch),
        compiler_params=pltpu.CompilerParams(vmem_limit_bytes=mib * 1024 * 1024),
    )(*operands)


def array(rows, width, dtype=BF16):
    return jax.ShapeDtypeStruct((rows, width), dtype)


def pack_body(ids_ref, weights_ref, tokens_ref, gain_ref, out_ref):
    rows, width = tokens_ref.shape
    values = tokens_ref[...].astype(F32)
    scaled = values * lax.rsqrt(jnp.mean(values * values, axis=-1, keepdims=True) + 1e-06)
    out_ref[0:rows, :] = (scaled * gain_ref[...].astype(F32)).astype(BF16)
    weights = weights_ref[...]
    first, second = weights[0:1], weights[1:2]
    both = first + second
    lines = [ids_ref[0:1].astype(F32), ids_ref[1:2].astype(F32)]
    for share in (first / both, second / both):
        high = share.astype(BF16).astype(F32)
        lines += [high, share - high]
    lines += [jnp.zeros_like(first)] * (META - len(lines))
    meta = jnp.concatenate(lines, axis=0)
    meta = jnp.concatenate([meta, jnp.zeros((META, width - rows), F32)], axis=1)
    out_ref[rows:, :] = meta.astype(BF16)


def slots_of(block_ref, place_ref, chips, sign, count, capacity, kept):
    rows = block_ref.shape[0] - META
    meta = block_ref[rows:, 0:rows].astype(F32)
    chip, core = place_ref[0], place_ref[1]
    index = lax.broadcasted_iota(jnp.int32, (count, rows), 0)
    step = lax.shift_right_logical(index, 1)
    first = 1 if sign else 0
    named = chip + sign * (first + step) + chips
    named = jnp.where(named >= chips, named - chips, named)
    named = jnp.where(named >= chips, named - chips, named)
    expert = (2 * named + ((core + (index & 1)) & 1)).astype(F32)
    is_first, is_second = meta[0:1] == expert, meta[1:2] == expert
    match = jnp.where(is_first, 1.0, 0.0) + jnp.where(is_second, 1.0, 0.0)
    shares = jnp.where(is_first, meta[2:3] + meta[3:4], 0.0) + jnp.where(
        is_second, meta[4:5] + meta[5:6], 0.0
    )
    upto = (
        lax.broadcasted_iota(jnp.int32, (rows, rows), 0)
        <= lax.broadcasted_iota(jnp.int32, (rows, rows), 1)
    ).astype(F32).astype(BF16)
    rank = jnp.dot(match.astype(BF16), upto, preferred_element_type=F32)
    slot = jnp.where(match > 0.5, rank - 1.0, -1.0)
    number = lax.broadcasted_iota(jnp.int32, (capacity, rows), 0).astype(F32)
    hot = [jnp.where(slot[e : e + 1] == number, 1.0, 0.0) for e in kept]
    return hot, [shares[e : e + 1] for e in kept]


def by_columns(width, body, pieces=4):
    @pl.loop(0, pieces)
    def _(i):
        body(pl.ds(pl.multiple_of(i * (width // pieces), 128), width // pieces))


def picked(chosen, block_ref, columns):
    rows = block_ref.shape[0] - META
    return jnp.dot(chosen, block_ref[0:rows, columns], preferred_element_type=F32).astype(BF16)


def weighed(hot, shares):
    values = [jnp.sum(h * s, axis=1, keepdims=True) for h, s in zip(hot, shares)]
    return jnp.concatenate(hot, axis=0).T.astype(BF16), values


def spread(chosen, values, results):
    scaled = [(v * r.astype(F32)).astype(BF16) for v, r in zip(values, results)]
    return jnp.dot(chosen, jnp.concatenate(scaled, axis=0), preferred_element_type=F32)


KEPT = {1: (0, 1, 2, 3, 4, 5, 6), -1: (0, 1, 2, 3, 4, 5, 7)}


def far_cuts(capacity):
    return [(2 * capacity * k, 2 * capacity * k + 2 * capacity) for k in range(3)] + [
        (6 * capacity, 7 * capacity)
    ]


def relay_body(chips, capacity, place_ref, up_ref, down_ref, *outs):
    todo = []
    for sign, block_ref, own in ((1, up_ref, outs[:4]), (-1, down_ref, outs[4:])):
        hot, _ = slots_of(block_ref, place_ref, chips, sign, 8, capacity, KEPT[sign])
        todo.append((jnp.concatenate(hot, axis=0).astype(BF16), block_ref, own))

    def piece(columns):
        for chosen, block_ref, own in todo:
            rows = picked(chosen, block_ref, columns)
            for (low, high), out_ref in zip(far_cuts(capacity), own):
                out_ref[:, columns] = rows[low:high]

    by_columns(up_ref.shape[1], piece)


def near_body(chips, capacity, place_ref, *refs):
    blocks, (same_ref, other_ref) = refs[:-2], refs[-2:]
    chosen = []
    for block_ref in blocks:
        hot, _ = slots_of(block_ref, place_ref, chips, 0, 8, capacity, (0, 1))
        chosen.append(jnp.concatenate(hot, axis=0).astype(BF16))

    def piece(columns):
        for i, block_ref in enumerate(blocks):
            rows = picked(chosen[i], block_ref, columns)
            same_ref[i * capacity : (i + 1) * capacity, columns] = rows[:capacity]
            other_ref[i * capacity : (i + 1) * capacity, columns] = rows[capacity:]

    by_columns(same_ref.shape[1], piece)


def unpack_body(capacity, *refs):
    far, (same_ref, other_ref) = refs[:-2], refs[-2:]
    same = [far[i][0:capacity, :] for i in (0, 1, 2, 3, 4, 5, 6)]
    other = [far[i][capacity : 2 * capacity, :] for i in (0, 1, 2, 4, 5, 6)] + [far[7][...]]
    for i in range(7):
        same_ref[i * capacity : (i + 1) * capacity, :] = same[i]
        other_ref[i * capacity : (i + 1) * capacity, :] = other[i]


def hidden_body(count, pairs, *refs):
    parts, weights, out_ref, rows_ref = refs[:count], refs[count : count + 2 * pairs], refs[-2], refs[-1]
    low = 0
    for ref in parts:
        rows_ref[low : low + ref.shape[0], :] = ref[...]
        low += ref.shape[0]

    @pl.loop(0, 2)
    def _(i):
        here = pl.ds(pl.multiple_of(i * (low // 2), 128), low // 2)
        for k in range(pairs):
            gate = jnp.dot(rows_ref[here, :], weights[2 * k][...], preferred_element_type=F32)
            upper = jnp.dot(rows_ref[here, :], weights[2 * k + 1][...], preferred_element_type=F32)
            made = (gate / (1.0 + jnp.exp(-gate)) * upper).astype(BF16)
            columns = made.shape[1]
            out_ref[here, k * columns : (k + 1) * columns] = made


def down_body(first, sizes, count, *refs):
    rows = sum(sizes)
    hidden = jnp.concatenate([ref[first : first + rows, :] for ref in refs[:count]], axis=1)
    outs = refs[len(refs) - len(sizes) :]
    weights = refs[count : len(refs) - len(sizes)]

    def piece(columns):
        total, low = 0.0, 0
        for ref in weights:
            total = total + jnp.dot(
                hidden[:, low : low + ref.shape[0]], ref[:, columns], preferred_element_type=F32
            )
            low += ref.shape[0]
        at = 0
        for size, out_ref in zip(sizes, outs):
            out_ref[:, columns] = total[at : at + size].astype(BF16)
            at += size

    by_columns(outs[0].shape[1], piece)


def far_back_body(capacity, same_ref, other_ref, *outs):
    for i in range(3):
        for base, own in ((0, outs[:4]), (4, outs[4:])):
            j = i + base
            k = i if base == 0 else i + 3
            own[i][0:capacity, :] = same_ref[j * capacity : (j + 1) * capacity, :]
            own[i][capacity:, :] = other_ref[k * capacity : (k + 1) * capacity, :]
    outs[3][...] = same_ref[3 * capacity : 4 * capacity, :]
    outs[7][...] = other_ref[6 * capacity : 7 * capacity, :]


def own_weighed(block_ref, place_ref, chips, capacity):
    return weighed(*slots_of(block_ref, place_ref, chips, 0, 8, capacity, (0, 1)))


def own_part(made, i, capacity, same_ref, other_ref, columns):
    low, high = i * capacity, (i + 1) * capacity
    return spread(*made, [same_ref[low:high, columns], other_ref[low:high, columns]])


def turn_body(chips, capacity, at, place_ref, up_ref, down_ref, same_ref, other_ref, *refs):
    far, outs = refs[:8], refs[8:]
    todo = []
    for sign, block_ref, own, i, out_ref in (
        (1, up_ref, far[:4], at[0], outs[0]),
        (-1, down_ref, far[4:], at[1], outs[1]),
    ):
        made = weighed(*slots_of(block_ref, place_ref, chips, sign, 8, capacity, KEPT[sign]))
        near = own_weighed(block_ref, place_ref, chips, capacity)
        todo.append((made, near, own, i, out_ref))

    def piece(columns):
        for made, near, own, i, out_ref in todo:
            results = []
            for ref in own:
                for low in range(0, ref.shape[0], capacity):
                    results.append(ref[low : low + capacity, columns])
            total = spread(*made, results)
            total = total + own_part(near, i, capacity, same_ref, other_ref, columns)
            out_ref[:, columns] = total.astype(BF16)

    by_columns(up_ref.shape[1], piece)


def near_back_body(chips, capacity, count, place_ref, *refs):
    blocks = refs[:count]
    same_ref, other_ref = refs[count : count + 2]
    outs = refs[count + 2 :]
    near = [own_weighed(block_ref, place_ref, chips, capacity) for block_ref in blocks]

    def piece(columns):
        for i, out_ref in enumerate(outs):
            total = own_part(near[i], i, capacity, same_ref, other_ref, columns)
            out_ref[:, columns] = total.astype(BF16)

    by_columns(same_ref.shape[1], piece)


def mixer_norm_body(tokens_ref, gain_ref, _, out_ref):
    values = tokens_ref[...].astype(F32)
    scaled = values * lax.rsqrt(jnp.mean(values * values, axis=-1, keepdims=True) + 1e-06)
    out_ref[...] = (scaled * gain_ref[...].astype(F32)).astype(BF16)


def mixer_first_body(members, place_ref, *refs):
    blocks, weight_ref, out_ref = refs[:members], refs[members], refs[members + 1]
    rows = blocks[0].shape[0]
    for k, block_ref in enumerate(blocks):
        at = lax.rem(place_ref[2] + k, members) * rows
        made = jnp.dot(block_ref[...], weight_ref[...], preferred_element_type=F32)
        out_ref[pl.ds(pl.multiple_of(at, rows), rows), :] = made.astype(BF16)


def mixer_second_body(members, place_ref, rim_ref, rows_ref, group_ref, scale_ref, weight_ref, *refs):
    outs, extended_ref = refs[:members], refs[members]
    rim, total = rim_ref.shape[0], rows_ref.shape[0]
    rows = total // members
    extended_ref[0:rim, :] = rim_ref[...]
    extended_ref[rim:, :] = rows_ref[...]
    window = lax.shift_left(jnp.int32(2), place_ref[2])
    behind = (
        lax.broadcasted_iota(jnp.int32, (rows, rows + rim), 0)
        - lax.broadcasted_iota(jnp.int32, (rows, rows + rim), 1)
        + rim
    )
    inside = jnp.where((behind >= 0) & (behind < window), 1.0, 0.0).astype(BF16)
    grouped = []
    for k in range(members):
        at = pl.multiple_of(lax.rem(place_ref[2] + k, members) * rows, rows)
        values = rows_ref[pl.ds(at, rows), :].astype(F32)
        sums = jnp.dot(
            inside, extended_ref[pl.ds(at, rows + rim), :], preferred_element_type=F32
        )
        position = place_ref[3] * total + at + 1 + lax.broadcasted_iota(jnp.int32, (rows, 1), 0)
        counts = jnp.minimum(position, window).astype(F32)
        pooled = (sums / counts - values).astype(BF16)
        made = jnp.dot(pooled, group_ref[...], preferred_element_type=F32)
        grouped.append((made * scale_ref[...].astype(F32)).astype(BF16))
    grouped = jnp.concatenate(grouped, axis=0)

    def piece(columns):
        made = jnp.dot(grouped, weight_ref[:, columns], preferred_element_type=F32).astype(BF16)
        for k, out_ref in enumerate(outs):
            out_ref[:, columns] = made[k * rows : (k + 1) * rows]

    by_columns(weight_ref.shape[1], piece)


def summed(*values):
    total = values[0].astype(F32)
    for value in values[1:]:
        total = total + value.astype(F32)
    return total.astype(BF16)


def mixer(
    place, mixer_tokens, mixer_gain, in_weight, group_weight, channel_scale, out_weight, wait
):
    rows, width = mixer_tokens.shape
    members = lax.axis_size("tp")
    columns = in_weight.shape[1]
    normed = call(
        6,
        mixer_norm_body,
        array(rows, width),
        mixer_tokens,
        mixer_gain[None],
        wait,
        scalars=0,
        waits=1,
    )
    blocks = [normed] + [rotated(normed, "tp", -k) for k in range(1, members)]
    pooled_in = call(
        12,
        functools.partial(mixer_first_body, members),
        array(rows * members, columns),
        place,
        *blocks,
        in_weight,
    )
    rim = shifted(pooled_in[rows * members - WINDOW_MAX :], "ep", 1)
    parts = call(
        16,
        functools.partial(mixer_second_body, members),
        [array(rows, width)] * members,
        place,
        rim,
        pooled_in,
        group_weight[0],
        channel_scale[None],
        out_weight,
        scratch=[pltpu.VMEM((rows * members + WINDOW_MAX, columns), BF16)],
    )
    parts = [parts[0]] + [rotated(parts[k], "tp", k) for k in range(1, members)]
    return summed(*parts)


def local(
    mixer_tokens,
    mixer_gain,
    in_weight,
    group_weight,
    channel_scale,
    out_weight,
    expert_tokens,
    expert_gain,
    route_ids,
    route_weights,
    gate_weight,
    up_weight,
    down_weight,
):
    rows, width = expert_tokens.shape
    chips = lax.axis_size("ep") // 2
    capacity = 4 * rows // (2 * chips)
    side = lax.axis_index("ep")
    place = jnp.stack([side // 2, side % 2, lax.axis_index("tp"), side]).astype(jnp.int32)
    block_rows = rows + META

    gates, uppers = gate_weight[0], up_weight[0]
    half = down_weight.shape[1] // 2
    halves = (down_weight[0, :half], down_weight[0, half:])
    gate_left, gate_right = rotated(gates, "tp", 1), rotated(gates, "tp", -1)
    upper_left, upper_right = rotated(uppers, "tp", 1), rotated(uppers, "tp", -1)
    downs_left = [rotated(w, "tp", 1) for w in halves]
    downs_right = [rotated(w, "tp", -1) for w in halves]
    gate_last = rotated(gate_left, "tp", 1)
    upper_last = rotated(upper_right, "tp", -1)
    downs_last = [rotated(downs_left[0], "tp", 1), rotated(downs_right[1], "tp", -1)]

    block = call(
        6,
        pack_body,
        array(block_rows, width),
        route_ids.T,
        route_weights.T,
        expert_tokens,
        expert_gain[None],
        scalars=0,
    )
    ups, downs = [block], [block]
    for _ in range(4):
        ups.append(rotated(ups[-1], "ep", 2))
        downs.append(rotated(downs[-1], "ep", -2))
    pieces = [array(high - low, width) for low, high in far_cuts(capacity)]
    far = call(
        8, functools.partial(relay_body, chips, capacity), pieces * 2, place, ups[4], downs[4]
    )
    far = [rotated(far[k], "ep", 2 * (k + 1)) for k in range(4)] + [
        rotated(far[4 + k], "ep", -2 * (k + 1)) for k in range(4)
    ]
    blocks = [block] + ups[1:4] + downs[1:4] + [ups[4], downs[4]]
    near_same, near_other = call(
        12,
        functools.partial(near_body, chips, capacity),
        [array(9 * capacity, width)] * 2,
        place,
        *blocks,
    )
    near_other = swapped(near_other, "ep")
    far_same, far_other = call(
        6,
        functools.partial(unpack_body, capacity),
        [array(7 * capacity, width)] * 2,
        *far,
        scalars=0,
    )
    far_other = swapped(far_other, "ep")

    parts = [far_same, far_other, near_same, near_other]
    sizes = [p.shape[0] for p in parts]
    total = sum(sizes)
    ff = gates.shape[1]
    rows_scratch = [pltpu.VMEM((total, width), BF16)]
    hidden = call(
        24,
        functools.partial(hidden_body, 4, 3),
        array(total, 3 * ff),
        *parts,
        gates,
        uppers,
        gate_left,
        upper_left,
        gate_right,
        upper_right,
        scalars=0,
        scratch=rows_scratch,
    )
    hidden_last = call(
        16,
        functools.partial(hidden_body, 4, 1),
        array(total, ff),
        *parts,
        gate_last,
        upper_last,
        hidden,
        scalars=0,
        waits=1,
        scratch=rows_scratch,
    )

    def results(first, sizes):
        return call(
            16,
            functools.partial(down_body, first, sizes, 2),
            [array(size, width) for size in sizes],
            hidden,
            hidden_last,
            down_weight[0],
            *downs_left,
            *downs_right,
            *downs_last,
            scalars=0,
        )

    far_same, far_other = results(0, sizes[:2])
    near_same, near_other = results(sum(sizes[:2]), sizes[2:])

    far_other = swapped(far_other, "ep")
    near_other = swapped(near_other, "ep")
    back = call(
        6, functools.partial(far_back_body, capacity), pieces * 2, far_same, far_other, scalars=0
    )
    back = [rotated(back[k], "ep", -2 * (k + 1)) for k in range(4)] + [
        rotated(back[4 + k], "ep", 2 * (k + 1)) for k in range(4)
    ]
    kept = call(
        16,
        functools.partial(near_back_body, chips, capacity, 7),
        [array(rows, width)] * 7,
        place,
        *blocks[:7],
        near_same,
        near_other,
    )
    up_sum, down_sum = call(
        10,
        functools.partial(turn_body, chips, capacity, (7, 8)),
        [array(rows, width)] * 2,
        place,
        ups[4],
        downs[4],
        near_same,
        near_other,
        *back,
    )
    for k in (3, 2, 1, 0):
        up_sum = rotated(up_sum, "ep", -2)
        down_sum = rotated(down_sum, "ep", 2)
        if k > 0:
            up_sum = summed(up_sum, kept[k])
            down_sum = summed(down_sum, kept[3 + k])
    expert_mix = summed(up_sum, down_sum, kept[0])

    mixed_tokens = mixer(
        place,
        mixer_tokens,
        mixer_gain,
        in_weight,
        group_weight,
        channel_scale,
        out_weight,
        hidden_last,
    )
    return (mixed_tokens, expert_mix)


def solution(mesh):
    placed = (
        P(("grp", "ep", "tp"), None),
        P(),
        P(None, "tp"),
        P("tp", None, None),
        P("tp"),
        P("tp", None),
        P(("grp", "ep", "tp"), None),
        P(),
        P(("grp", "ep", "tp"), None),
        P(("grp", "ep", "tp"), None),
        P("ep", None, "tp"),
        P("ep", None, "tp"),
        P("ep", "tp", None),
    )

    return jax.shard_map(
        local,
        mesh=mesh,
        in_specs=placed,
        out_specs=(P(("grp", "ep", "tp"), None), P(("grp", "ep", "tp"), None)),
        check_vma=False,
    )
```

```python
import functools

import jax
import jax.numpy as jnp
from jax import lax
from jax.experimental import pallas as pl
from jax.experimental.pallas import tpu as pltpu
from jax.sharding import PartitionSpec as P


WINDOW_MAX = 16
META = 8
F32 = jnp.float32
BF16 = jnp.bfloat16


def shifted(value, axis, by):
    devices = lax.axis_size(axis)
    pairs = [(i, i + by) for i in range(devices) if 0 <= i + by < devices]
    return lax.ppermute(value, axis, pairs)


def rotated(value, axis, by):
    devices = lax.axis_size(axis)
    return lax.ppermute(value, axis, [(i, (i + by) % devices) for i in range(devices)])


def swapped(value, axis):
    devices = lax.axis_size(axis)
    return lax.ppermute(value, axis, [(i, i ^ 1) for i in range(devices)])


def call(mib, body, outs, *operands, scalars=1, waits=0, scratch=()):
    specs = (
        [pl.BlockSpec(memory_space=pltpu.SMEM)] * scalars
        + [pl.BlockSpec(memory_space=pltpu.VMEM)] * (len(operands) - scalars - waits)
        + [pl.BlockSpec(memory_space=pl.ANY)] * waits
    )
    return pl.pallas_call(
        body,
        out_shape=outs,
        in_specs=specs,
        out_specs=jax.tree.map(lambda _: pl.BlockSpec(memory_space=pltpu.VMEM), outs),
        scratch_shapes=list(scratch),
        compiler_params=pltpu.CompilerParams(vmem_limit_bytes=mib * 1024 * 1024),
    )(*operands)


def array(rows, width, dtype=BF16):
    return jax.ShapeDtypeStruct((rows, width), dtype)


def pack_body(ids_ref, weights_ref, tokens_ref, gain_ref, out_ref):
    rows, width = tokens_ref.shape
    values = tokens_ref[...].astype(F32)
    scaled = values * lax.rsqrt(jnp.mean(values * values, axis=-1, keepdims=True) + 1e-06)
    out_ref[0:rows, :] = (scaled * gain_ref[...].astype(F32)).astype(BF16)
    weights = weights_ref[...]
    first, second = weights[0:1], weights[1:2]
    both = first + second
    lines = [ids_ref[0:1].astype(F32), ids_ref[1:2].astype(F32)]
    for share in (first / both, second / both):
        high = share.astype(BF16).astype(F32)
        lines += [high, share - high]
    lines += [jnp.zeros_like(first)] * (META - len(lines))
    meta = jnp.concatenate(lines, axis=0)
    meta = jnp.concatenate([meta, jnp.zeros((META, width - rows), F32)], axis=1)
    out_ref[rows:, :] = meta.astype(BF16)


def slots_of(block_ref, place_ref, chips, sign, count, capacity, kept):
    rows = block_ref.shape[0] - META
    meta = block_ref[rows:, 0:rows].astype(F32)
    chip, core = place_ref[0], place_ref[1]
    index = lax.broadcasted_iota(jnp.int32, (count, rows), 0)
    step = lax.shift_right_logical(index, 1)
    first = 1 if sign else 0
    named = chip + sign * (first + step) + chips
    named = jnp.where(named >= chips, named - chips, named)
    named = jnp.where(named >= chips, named - chips, named)
    expert = (2 * named + ((core + (index & 1)) & 1)).astype(F32)
    is_first, is_second = meta[0:1] == expert, meta[1:2] == expert
    match = jnp.where(is_first, 1.0, 0.0) + jnp.where(is_second, 1.0, 0.0)
    shares = jnp.where(is_first, meta[2:3] + meta[3:4], 0.0) + jnp.where(
        is_second, meta[4:5] + meta[5:6], 0.0
    )
    upto = (
        lax.broadcasted_iota(jnp.int32, (rows, rows), 0)
        <= lax.broadcasted_iota(jnp.int32, (rows, rows), 1)
    ).astype(F32).astype(BF16)
    rank = jnp.dot(match.astype(BF16), upto, preferred_element_type=F32)
    slot = jnp.where(match > 0.5, rank - 1.0, -1.0)
    number = lax.broadcasted_iota(jnp.int32, (capacity, rows), 0).astype(F32)
    hot = [jnp.where(slot[e : e + 1] == number, 1.0, 0.0) for e in kept]
    return hot, [shares[e : e + 1] for e in kept]


def by_columns(width, body, pieces=8):
    @pl.loop(0, pieces)
    def _(i):
        body(pl.ds(pl.multiple_of(i * (width // pieces), 128), width // pieces))


def picked(chosen, block_ref, columns):
    rows = block_ref.shape[0] - META
    return jnp.dot(chosen, block_ref[0:rows, columns], preferred_element_type=F32).astype(BF16)


def weighed(hot, shares):
    values = [jnp.sum(h * s, axis=1, keepdims=True) for h, s in zip(hot, shares)]
    return jnp.concatenate(hot, axis=0).T.astype(BF16), values


def spread(chosen, values, results):
    scaled = [(v * r.astype(F32)).astype(BF16) for v, r in zip(values, results)]
    return jnp.dot(chosen, jnp.concatenate(scaled, axis=0), preferred_element_type=F32)


KEPT = {1: (0, 1, 2, 3, 4, 5, 6), -1: (0, 1, 2, 3, 4, 5, 7)}


def far_cuts(capacity):
    return [(2 * capacity * k, 2 * capacity * k + 2 * capacity) for k in range(3)] + [
        (6 * capacity, 7 * capacity)
    ]


def relay_body(chips, capacity, place_ref, up_ref, down_ref, *outs):
    todo = []
    for sign, block_ref, own in ((1, up_ref, outs[:2]), (-1, down_ref, outs[2:])):
        kept = (0, 1, 2 if sign > 0 else 3)
        hot, _ = slots_of(block_ref, place_ref, chips, sign, 8, capacity, kept)
        todo.append((jnp.concatenate(hot, axis=0).astype(BF16), block_ref, own))

    def piece(columns):
        for chosen, block_ref, (one_ref, two_ref) in todo:
            rows = picked(chosen, block_ref, columns)
            one_ref[:, columns] = rows[: 2 * capacity]
            two_ref[:, columns] = rows[2 * capacity :]

    by_columns(up_ref.shape[1], piece)


def blocks_of(ups_ref, downs_ref, up_ref, down_ref):
    ups = [ups_ref.at[i] for i in range(ups_ref.shape[0])] + [up_ref]
    downs = [downs_ref.at[i] for i in range(downs_ref.shape[0])] + [down_ref]
    return ups[0:4] + downs[1:4] + [ups[4], downs[4]] + ups[5:7] + downs[5:7]


def near_body(chips, capacity, place_ref, ups_ref, downs_ref, up_ref, down_ref, same_ref, other_ref):
    blocks = blocks_of(ups_ref, downs_ref, up_ref, down_ref)
    chosen = []
    for block_ref in blocks:
        hot, _ = slots_of(block_ref, place_ref, chips, 0, 8, capacity, (0, 1))
        chosen.append(jnp.concatenate(hot, axis=0).astype(BF16))

    def piece(columns):
        for i, block_ref in enumerate(blocks):
            rows = picked(chosen[i], block_ref, columns)
            same_ref[i * capacity : (i + 1) * capacity, columns] = rows[:capacity]
            other_ref[i * capacity : (i + 1) * capacity, columns] = rows[capacity:]

    by_columns(same_ref.shape[1], piece)


def unpack_body(capacity, near_ref, up_one, up_two, down_one, down_two, same_ref, other_ref):
    one, two, three = (slice(i * capacity, (i + 1) * capacity) for i in range(3))
    same_ref[one, :] = up_one[one, :]
    same_ref[two, :] = up_two[...]
    same_ref[three, :] = down_one[one, :]
    low = near_ref.shape[0]
    other_ref[0:low, :] = near_ref[...]
    other_ref[low : low + capacity, :] = up_one[two, :]
    other_ref[low + capacity : low + 2 * capacity, :] = down_one[two, :]
    other_ref[low + 2 * capacity :, :] = down_two[...]


FAR_SAME = ((0, 9), (0, 10), (1, 0), (1, 1), (0, 11), (0, 12), (1, 2))
FAR_OTHER = ((2, 9), (2, 10), (2, 13), (2, 11), (2, 12), (2, 14), (2, 15))
NEAR_SAME = tuple((0, i) for i in range(9))
NEAR_OTHER = tuple((2, i) for i in range(9))


def hidden_body(capacity, pairs, near_same, far_same, other, *refs):
    weights, out_ref, rows_ref = refs[: 2 * pairs], refs[-2], refs[-1]
    sources, low = (near_same, far_same, other), 0
    for which, i in FAR_SAME + FAR_OTHER + NEAR_SAME + NEAR_OTHER:
        rows_ref[low : low + capacity, :] = sources[which][i * capacity : (i + 1) * capacity, :]
        low += capacity

    @pl.loop(0, 4)
    def _(i):
        here = pl.ds(pl.multiple_of(i * (low // 4), 128), low // 4)
        for k in range(pairs):
            gate = jnp.dot(rows_ref[here, :], weights[2 * k][...], preferred_element_type=F32)
            upper = jnp.dot(rows_ref[here, :], weights[2 * k + 1][...], preferred_element_type=F32)
            made = (gate / (1.0 + jnp.exp(-gate)) * upper).astype(BF16)
            columns = made.shape[1]
            out_ref[here, k * columns : (k + 1) * columns] = made


def down_body(first, sizes, count, *refs):
    rows = sum(sizes)
    hidden = jnp.concatenate([ref[first : first + rows, :] for ref in refs[:count]], axis=1)
    outs = refs[len(refs) - len(sizes) :]
    weights = refs[count : len(refs) - len(sizes)]

    def piece(columns):
        total, low = 0.0, 0
        for ref in weights:
            total = total + jnp.dot(
                hidden[:, low : low + ref.shape[0]], ref[:, columns], preferred_element_type=F32
            )
            low += ref.shape[0]
        at = 0
        for size, out_ref in zip(sizes, outs):
            out_ref[:, columns] = total[at : at + size].astype(BF16)
            at += size

    by_columns(outs[0].shape[1], piece)


def far_back_body(capacity, same_ref, other_ref, *outs):
    for i in range(3):
        for base, own in ((0, outs[:4]), (4, outs[4:])):
            j = i + base
            k = i if base == 0 else i + 3
            own[i][0:capacity, :] = same_ref[j * capacity : (j + 1) * capacity, :]
            own[i][capacity:, :] = other_ref[k * capacity : (k + 1) * capacity, :]
    outs[3][...] = same_ref[3 * capacity : 4 * capacity, :]
    outs[7][...] = other_ref[6 * capacity : 7 * capacity, :]


def own_weighed(block_ref, place_ref, chips, capacity):
    return weighed(*slots_of(block_ref, place_ref, chips, 0, 8, capacity, (0, 1)))


def own_part(made, i, capacity, same_ref, other_ref, columns):
    low, high = i * capacity, (i + 1) * capacity
    return spread(*made, [same_ref[low:high, columns], other_ref[low:high, columns]])


def turn_body(chips, capacity, at, place_ref, ups_ref, downs_ref, same_ref, other_ref, *refs):
    far, outs = refs[:8], refs[8:]
    up_ref, down_ref = ups_ref.at[4], downs_ref.at[4]
    todo = []
    for sign, block_ref, own, i, out_ref in (
        (1, up_ref, far[:4], at[0], outs[0]),
        (-1, down_ref, far[4:], at[1], outs[1]),
    ):
        made = weighed(*slots_of(block_ref, place_ref, chips, sign, 8, capacity, KEPT[sign]))
        near = own_weighed(block_ref, place_ref, chips, capacity)
        todo.append((made, near, own, i, out_ref))

    def piece(columns):
        for made, near, own, i, out_ref in todo:
            results = []
            for ref in own:
                for low in range(0, ref.shape[0], capacity):
                    results.append(ref[low : low + capacity, columns])
            total = spread(*made, results)
            total = total + own_part(near, i, capacity, same_ref, other_ref, columns)
            out_ref[:, columns] = total.astype(BF16)

    by_columns(up_ref.shape[1], piece)


def near_back_body(chips, capacity, place_ref, ups_ref, downs_ref, same_ref, other_ref, *outs):
    blocks = [ups_ref.at[i] for i in range(4)] + [downs_ref.at[i] for i in range(1, 4)]
    near = [own_weighed(block_ref, place_ref, chips, capacity) for block_ref in blocks]

    def piece(columns):
        for i, out_ref in enumerate(outs):
            total = own_part(near[i], i, capacity, same_ref, other_ref, columns)
            out_ref[:, columns] = total.astype(BF16)

    by_columns(same_ref.shape[1], piece)


def mixer_norm_body(tokens_ref, gain_ref, _, out_ref):
    values = tokens_ref[...].astype(F32)
    scaled = values * lax.rsqrt(jnp.mean(values * values, axis=-1, keepdims=True) + 1e-06)
    out_ref[...] = (scaled * gain_ref[...].astype(F32)).astype(BF16)


def mixer_first_body(members, place_ref, *refs):
    blocks, weight_ref, out_ref, held_ref = refs[:members], *refs[members:]
    rows = blocks[0].shape[0]
    for k, block_ref in enumerate(blocks):
        held_ref[k] = block_ref[...]

    @pl.loop(0, members)
    def _(k):
        at = lax.rem(place_ref[2] + k, members) * rows
        made = jnp.dot(held_ref[k], weight_ref[...], preferred_element_type=F32)
        out_ref[pl.ds(pl.multiple_of(at, rows), rows), :] = made.astype(BF16)


def mixer_second_body(
    place_ref, rim_ref, rows_ref, group_ref, scale_ref, weight_ref, out_ref, extended_ref, grouped_ref
):
    members, rows = out_ref.shape[0], out_ref.shape[1]
    rim, total = rim_ref.shape[0], rows_ref.shape[0]
    extended_ref[0:rim, :] = rim_ref[...]
    extended_ref[rim:, :] = rows_ref[...]
    window = lax.shift_left(jnp.int32(2), place_ref[2])
    behind = (
        lax.broadcasted_iota(jnp.int32, (rows, rows + rim), 0)
        - lax.broadcasted_iota(jnp.int32, (rows, rows + rim), 1)
        + rim
    )
    inside = jnp.where((behind >= 0) & (behind < window), 1.0, 0.0).astype(BF16)

    @pl.loop(0, members)
    def _(k):
        at = pl.multiple_of(k * rows, rows)
        values = rows_ref[pl.ds(at, rows), :].astype(F32)
        sums = jnp.dot(
            inside, extended_ref[pl.ds(at, rows + rim), :], preferred_element_type=F32
        )
        position = place_ref[3] * total + at + 1 + lax.broadcasted_iota(jnp.int32, (rows, 1), 0)
        counts = jnp.minimum(position, window).astype(F32)
        pooled = (sums / counts - values).astype(BF16)
        made = jnp.dot(pooled, group_ref[...], preferred_element_type=F32)
        grouped_ref[pl.ds(at, rows), :] = (made * scale_ref[...].astype(F32)).astype(BF16)

    def piece(columns):
        made = jnp.dot(grouped_ref[...], weight_ref[:, columns], preferred_element_type=F32)
        for k in range(members):
            out_ref[k, :, columns] = made[k * rows : (k + 1) * rows].astype(BF16)

    by_columns(weight_ref.shape[1], piece)


def sum_body(*refs):
    planes, out_ref = [], refs[-1]
    for ref in refs[:-1]:
        planes += [ref] if len(ref.shape) == 2 else [ref.at[i] for i in range(ref.shape[0])]
    pieces = 8
    rows = out_ref.shape[0] // pieces

    @pl.loop(0, pieces)
    def _(i):
        here = pl.ds(pl.multiple_of(i * rows, rows), rows)
        total = planes[0][here, :].astype(F32)
        for ref in planes[1:]:
            total = total + ref[here, :].astype(F32)
        out_ref[here, :] = total.astype(BF16)


def summed(*values):
    return call(6, sum_body, array(*values[0].shape[-2:]), *values, scalars=0)


def mixer(
    place, mixer_tokens, mixer_gain, in_weight, group_weight, channel_scale, out_weight, wait
):
    rows, width = mixer_tokens.shape
    members = lax.axis_size("tp")
    columns = in_weight.shape[1]
    normed = call(
        6,
        mixer_norm_body,
        array(rows, width),
        mixer_tokens,
        mixer_gain[None],
        wait,
        scalars=0,
        waits=1,
    )
    blocks = [normed] + [rotated(normed, "tp", -k) for k in range(1, members)]
    pooled_in = call(
        12,
        functools.partial(mixer_first_body, members),
        array(rows * members, columns),
        place,
        *blocks,
        in_weight,
        scratch=[pltpu.VMEM((members, rows, width), BF16)],
    )
    rim = shifted(pooled_in[rows * members - WINDOW_MAX :], "ep", 1)
    parts = call(
        16,
        mixer_second_body,
        jax.ShapeDtypeStruct((members, rows, width), BF16),
        place,
        rim,
        pooled_in,
        group_weight[0],
        channel_scale[None],
        out_weight,
        scratch=[
            pltpu.VMEM((rows * members + WINDOW_MAX, columns), BF16),
            pltpu.VMEM((rows * members, columns), BF16),
        ],
    )
    parts = lax.all_to_all(parts, "tp", 0, 0, tiled=True)
    return summed(parts)


def local(
    mixer_tokens,
    mixer_gain,
    in_weight,
    group_weight,
    channel_scale,
    out_weight,
    expert_tokens,
    expert_gain,
    route_ids,
    route_weights,
    gate_weight,
    up_weight,
    down_weight,
):
    rows, width = expert_tokens.shape
    chips = lax.axis_size("ep") // 2
    capacity = 4 * rows // (2 * chips)
    side = lax.axis_index("ep")
    place = jnp.stack([side // 2, side % 2, lax.axis_index("tp"), side]).astype(jnp.int32)
    block_rows = rows + META

    gates, uppers = gate_weight[0], up_weight[0]
    half = down_weight.shape[1] // 2
    gate_left, gate_right = rotated(gates, "tp", 1), rotated(gates, "tp", -1)
    upper_left, upper_right = rotated(uppers, "tp", 1), rotated(uppers, "tp", -1)
    down_left, down_right = rotated(down_weight[0], "tp", 1), rotated(down_weight[0], "tp", -1)
    gate_last = rotated(gate_left, "tp", 1)
    upper_last = rotated(upper_right, "tp", -1)
    downs_last = [rotated(down_left[:half], "tp", 1), rotated(down_right[half:], "tp", -1)]

    block = call(
        6,
        pack_body,
        array(block_rows, width),
        route_ids.T,
        route_weights.T,
        expert_tokens,
        expert_gain[None],
        scalars=0,
    )

    def step(held, _):
        up, down = held
        return (rotated(up, "ep", 2), rotated(down, "ep", -2)), held

    (up, down), (ups, downs) = lax.scan(step, (block, block), None, length=6)
    cut = [array(2 * capacity, width), array(capacity, width)]
    far = call(8, functools.partial(relay_body, chips, capacity), cut * 2, place, up, down)
    far = [
        rotated(far[0], "ep", 2),
        rotated(far[1], "ep", 4),
        rotated(far[2], "ep", -2),
        rotated(far[3], "ep", -4),
    ]
    near_same, near_other = call(
        16,
        functools.partial(near_body, chips, capacity),
        [array(13 * capacity, width)] * 2,
        place,
        ups,
        downs,
        up,
        down,
    )
    far_same, other = call(
        6,
        functools.partial(unpack_body, capacity),
        [array(3 * capacity, width), array(16 * capacity, width)],
        near_other,
        *far,
        scalars=0,
    )
    other = swapped(other, "ep")

    parts = [near_same, far_same, other]
    sizes = [7 * capacity] * 2 + [9 * capacity] * 2
    pieces = [array(high - low, width) for low, high in far_cuts(capacity)]
    total = sum(sizes)
    ff = gates.shape[1]
    rows_scratch = [pltpu.VMEM((total, width), BF16)]
    hidden = call(
        24,
        functools.partial(hidden_body, capacity, 3),
        array(total, 3 * ff),
        *parts,
        gates,
        uppers,
        gate_left,
        upper_left,
        gate_right,
        upper_right,
        scalars=0,
        scratch=rows_scratch,
    )
    hidden_last = call(
        16,
        functools.partial(hidden_body, capacity, 1),
        array(total, ff),
        *parts,
        gate_last,
        upper_last,
        hidden,
        scalars=0,
        waits=1,
        scratch=rows_scratch,
    )

    def results(first, sizes):
        return call(
            16,
            functools.partial(down_body, first, sizes, 2),
            [array(size, width) for size in sizes],
            hidden,
            hidden_last,
            down_weight[0],
            down_left,
            down_right,
            *downs_last,
            scalars=0,
        )

    far_same, far_other = results(0, sizes[:2])
    near_same, near_other = results(sum(sizes[:2]), sizes[2:])

    far_other = swapped(far_other, "ep")
    near_other = swapped(near_other, "ep")
    back = call(
        6, functools.partial(far_back_body, capacity), pieces * 2, far_same, far_other, scalars=0
    )
    back = [rotated(back[k], "ep", -2 * (k + 1)) for k in range(4)] + [
        rotated(back[4 + k], "ep", 2 * (k + 1)) for k in range(4)
    ]
    kept = call(
        16,
        functools.partial(near_back_body, chips, capacity),
        [array(rows, width)] * 7,
        place,
        ups,
        downs,
        near_same,
        near_other,
    )
    up_sum, down_sum = call(
        10,
        functools.partial(turn_body, chips, capacity, (7, 8)),
        [array(rows, width)] * 2,
        place,
        ups,
        downs,
        near_same,
        near_other,
        *back,
    )
    for k in (3, 2, 1, 0):
        up_sum = rotated(up_sum, "ep", -2)
        down_sum = rotated(down_sum, "ep", 2)
        if k > 0:
            up_sum = summed(up_sum, kept[k])
            down_sum = summed(down_sum, kept[3 + k])
    expert_mix = summed(up_sum, down_sum, kept[0])

    mixed_tokens = mixer(
        place,
        mixer_tokens,
        mixer_gain,
        in_weight,
        group_weight,
        channel_scale,
        out_weight,
        hidden_last,
    )
    return (mixed_tokens, expert_mix)


def solution(mesh):
    placed = (
        P(("grp", "ep", "tp"), None),
        P(),
        P(None, "tp"),
        P("tp", None, None),
        P("tp"),
        P("tp", None),
        P(("grp", "ep", "tp"), None),
        P(),
        P(("grp", "ep", "tp"), None),
        P(("grp", "ep", "tp"), None),
        P("ep", None, "tp"),
        P("ep", None, "tp"),
        P("ep", "tp", None),
    )

    return jax.shard_map(
        local,
        mesh=mesh,
        in_specs=placed,
        out_specs=(P(("grp", "ep", "tp"), None), P(("grp", "ep", "tp"), None)),
        check_vma=False,
    )
```

```python
import functools

import jax
import jax.numpy as jnp
from jax import lax
from jax.experimental import pallas as pl
from jax.experimental.pallas import tpu as pltpu
from jax.sharding import PartitionSpec as P


WINDOW_MAX = 16
META = 8
F32 = jnp.float32
BF16 = jnp.bfloat16


def shifted(value, axis, by):
    devices = lax.axis_size(axis)
    pairs = [(i, i + by) for i in range(devices) if 0 <= i + by < devices]
    return lax.ppermute(value, axis, pairs)


def exchanged(value, axis, phase, width=1):
    devices = lax.axis_size(axis)
    groups = devices // width
    pairs = []
    for i in range(devices):
        group, place = divmod(i, width)
        partner = (group + (1 if group % 2 == phase else -1)) % groups
        pairs.append((i, partner * width + place))
    return lax.ppermute(value, axis, pairs)


def thrown(value, by):
    devices = lax.axis_size("ep")
    pairs = [(i, (i + (2 * by if i // 2 % 2 == 0 else -2 * by)) % devices) for i in range(devices)]
    return lax.ppermute(value, "ep", pairs)


def returned(value, by):
    return thrown(value, by if by % 2 else -by)


def opposite(value, axis):
    devices = lax.axis_size(axis)
    return lax.ppermute(value, axis, [(i, (i + devices // 2) % devices) for i in range(devices)])


def swapped(value, axis):
    devices = lax.axis_size(axis)
    return lax.ppermute(value, axis, [(i, i ^ 1) for i in range(devices)])


def call(mib, body, outs, *operands, scalars=1, waits=0, scratch=()):
    specs = (
        [pl.BlockSpec(memory_space=pltpu.SMEM)] * scalars
        + [pl.BlockSpec(memory_space=pltpu.VMEM)] * (len(operands) - scalars - waits)
        + [pl.BlockSpec(memory_space=pl.ANY)] * waits
    )
    return pl.pallas_call(
        body,
        out_shape=outs,
        in_specs=specs,
        out_specs=jax.tree.map(lambda _: pl.BlockSpec(memory_space=pltpu.VMEM), outs),
        scratch_shapes=list(scratch),
        compiler_params=pltpu.CompilerParams(vmem_limit_bytes=mib * 1024 * 1024),
    )(*operands)


def array(rows, width, dtype=BF16):
    return jax.ShapeDtypeStruct((rows, width), dtype)


def normalized(tokens_ref, gain_ref, out_ref, size=16):
    @pl.loop(0, tokens_ref.shape[0] // size)
    def _(i):
        here = pl.ds(pl.multiple_of(i * size, size), size)
        values = tokens_ref[here, :].astype(F32)
        scaled = values * lax.rsqrt(jnp.mean(values * values, axis=-1, keepdims=True) + 1e-06)
        out_ref[here, :] = (scaled * gain_ref[...].astype(F32)).astype(BF16)


def pack_body(ids_ref, weights_ref, tokens_ref, gain_ref, out_ref):
    rows, width = tokens_ref.shape
    normalized(tokens_ref, gain_ref, out_ref)
    weights = weights_ref[...]
    first, second = weights[0:1], weights[1:2]
    both = first + second
    lines = [ids_ref[0:1].astype(F32), ids_ref[1:2].astype(F32)]
    for share in (first / both, second / both):
        high = share.astype(BF16).astype(F32)
        lines += [high, share - high]
    lines += [jnp.zeros_like(first)] * (META - len(lines))
    meta = jnp.concatenate(lines, axis=0)
    meta = jnp.concatenate([meta, jnp.zeros((META, width - rows), F32)], axis=1)
    out_ref[rows:, :] = meta.astype(BF16)


def slots_of(block_ref, place_ref, chips, sign, count, capacity, kept):
    rows = block_ref.shape[0] - META
    meta = block_ref[rows:, 0:rows].astype(F32)
    chip, core = place_ref[0], place_ref[1]
    index = lax.broadcasted_iota(jnp.int32, (count, rows), 0)
    step = lax.shift_right_logical(index, 1)
    away = sign * (1 - 2 * (chip & 1))
    named = chip + away * (1 + step) + chips if sign else chip + 0 * step
    named = jnp.where(named >= chips, named - chips, named)
    named = jnp.where(named >= chips, named - chips, named)
    expert = (2 * named + ((core + (index & 1)) & 1)).astype(F32)
    is_first, is_second = meta[0:1] == expert, meta[1:2] == expert
    match = jnp.where(is_first, 1.0, 0.0) + jnp.where(is_second, 1.0, 0.0)
    shares = jnp.where(is_first, meta[2:3] + meta[3:4], 0.0) + jnp.where(
        is_second, meta[4:5] + meta[5:6], 0.0
    )
    upto = (
        lax.broadcasted_iota(jnp.int32, (rows, rows), 0)
        <= lax.broadcasted_iota(jnp.int32, (rows, rows), 1)
    ).astype(F32).astype(BF16)
    rank = jnp.dot(match.astype(BF16), upto, preferred_element_type=F32)
    slot = jnp.where(match > 0.5, rank - 1.0, -1.0)
    number = lax.broadcasted_iota(jnp.int32, (capacity, rows), 0).astype(F32)
    hot = [jnp.where(slot[e : e + 1] == number, 1.0, 0.0) for e in kept]
    return hot, [shares[e : e + 1] for e in kept]


def by_columns(width, body, pieces=8):
    @pl.loop(0, pieces)
    def _(i):
        body(pl.ds(pl.multiple_of(i * (width // pieces), 128), width // pieces))


def picked(chosen, block_ref, columns):
    rows = block_ref.shape[0] - META
    return jnp.dot(chosen, block_ref[0:rows, columns], preferred_element_type=F32).astype(BF16)


def weighed(hot, shares):
    values = [jnp.sum(h * s, axis=1, keepdims=True) for h, s in zip(hot, shares)]
    return jnp.concatenate(hot, axis=0).T.astype(BF16), values


def spread(chosen, values, results):
    scaled = [(v * r.astype(F32)).astype(BF16) for v, r in zip(values, results)]
    return jnp.dot(chosen, jnp.concatenate(scaled, axis=0), preferred_element_type=F32)


KEPT = {1: (0, 1, 2, 3, 4, 5, 6), -1: (0, 1, 2, 3, 4, 5, 7)}


def far_cuts(capacity):
    return [(2 * capacity * k, 2 * capacity * k + 2 * capacity) for k in range(3)] + [
        (6 * capacity, 7 * capacity)
    ]


def relay_body(chips, capacity, place_ref, up_ref, down_ref, *outs):
    todo = []
    for sign, block_ref, own in ((1, up_ref, outs[:4]), (-1, down_ref, outs[4:])):
        hot, _ = slots_of(block_ref, place_ref, chips, sign, 8, capacity, KEPT[sign])
        todo.append((jnp.concatenate(hot, axis=0).astype(BF16), block_ref, own))

    def piece(columns):
        for chosen, block_ref, own in todo:
            rows = picked(chosen, block_ref, columns)
            for (low, high), out_ref in zip(far_cuts(capacity), own):
                out_ref[:, columns] = rows[low:high]

    by_columns(up_ref.shape[1], piece)


def near_body(chips, capacity, place_ref, *refs):
    blocks, (same_ref, other_ref) = refs[:-2], refs[-2:]
    chosen = []
    for block_ref in blocks:
        hot, _ = slots_of(block_ref, place_ref, chips, 0, 8, capacity, (0, 1))
        chosen.append(jnp.concatenate(hot, axis=0).astype(BF16))

    def piece(columns):
        for i, block_ref in enumerate(blocks):
            rows = picked(chosen[i], block_ref, columns)
            same_ref[i * capacity : (i + 1) * capacity, columns] = rows[:capacity]
            other_ref[i * capacity : (i + 1) * capacity, columns] = rows[capacity:]

    by_columns(same_ref.shape[1], piece)


def unpack_body(capacity, near_ref, *refs):
    far, (same_ref, other_ref) = refs[:-2], refs[-2:]
    low = near_ref.shape[0]
    other_ref[0:low, :] = near_ref[...]
    for i in range(7):
        here = slice(i * capacity, (i + 1) * capacity)
        same_ref[here, :] = far[i][0:capacity, :]
    for i, k in enumerate((0, 1, 2, 4, 5, 6)):
        at = low + i * capacity
        other_ref[at : at + capacity, :] = far[k][capacity : 2 * capacity, :]
    other_ref[low + 6 * capacity :, :] = far[7][...]


def hidden_body(pairs, far_same, near_same, other, *refs):
    weights, out_ref, rows_ref = refs[: 2 * pairs], refs[-2], refs[-1]
    near, far = near_same.shape[0], far_same.shape[0]
    rows_ref[0:far, :] = far_same[...]
    rows_ref[far : 2 * far, :] = other[near:, :]
    rows_ref[2 * far : 2 * far + near, :] = near_same[...]
    rows_ref[2 * far + near :, :] = other[0:near, :]
    low = rows_ref.shape[0]

    @pl.loop(0, 4)
    def _(i):
        here = pl.ds(pl.multiple_of(i * (low // 4), 128), low // 4)
        for k in range(pairs):
            gate = jnp.dot(rows_ref[here, :], weights[2 * k][...], preferred_element_type=F32)
            upper = jnp.dot(rows_ref[here, :], weights[2 * k + 1][...], preferred_element_type=F32)
            made = (gate / (1.0 + jnp.exp(-gate)) * upper).astype(BF16)
            columns = made.shape[1]
            out_ref[here, k * columns : (k + 1) * columns] = made


def down_body(first, sizes, count, *refs):
    rows = sum(sizes)
    hidden = jnp.concatenate([ref[first : first + rows, :] for ref in refs[:count]], axis=1)
    outs = refs[len(refs) - len(sizes) :]
    weights = refs[count : len(refs) - len(sizes)]

    def piece(columns):
        total, low = 0.0, 0
        for ref in weights:
            total = total + jnp.dot(
                hidden[:, low : low + ref.shape[0]], ref[:, columns], preferred_element_type=F32
            )
            low += ref.shape[0]
        at = 0
        for size, out_ref in zip(sizes, outs):
            out_ref[:, columns] = total[at : at + size].astype(BF16)
            at += size

    by_columns(outs[0].shape[1], piece)


def far_back_body(capacity, same_ref, other_ref, *outs):
    for i in range(3):
        for base, own in ((0, outs[:4]), (4, outs[4:])):
            j = i + base
            k = i if base == 0 else i + 3
            own[i][0:capacity, :] = same_ref[j * capacity : (j + 1) * capacity, :]
            own[i][capacity:, :] = other_ref[k * capacity : (k + 1) * capacity, :]
    outs[3][...] = same_ref[3 * capacity : 4 * capacity, :]
    outs[7][...] = other_ref[6 * capacity : 7 * capacity, :]


def own_weighed(block_ref, place_ref, chips, capacity):
    return weighed(*slots_of(block_ref, place_ref, chips, 0, 8, capacity, (0, 1)))


def own_part(made, i, capacity, same_ref, other_ref, columns):
    low, high = i * capacity, (i + 1) * capacity
    return spread(*made, [same_ref[low:high, columns], other_ref[low:high, columns]])


def turn_body(chips, capacity, at, place_ref, up_ref, down_ref, same_ref, other_ref, *refs):
    far, outs = refs[:8], refs[8:]
    todo = []
    for sign, block_ref, own, i, out_ref in (
        (1, up_ref, far[:4], at[0], outs[0]),
        (-1, down_ref, far[4:], at[1], outs[1]),
    ):
        made = weighed(*slots_of(block_ref, place_ref, chips, sign, 8, capacity, KEPT[sign]))
        near = own_weighed(block_ref, place_ref, chips, capacity)
        todo.append((made, near, own, i, out_ref))

    def piece(columns):
        for made, near, own, i, out_ref in todo:
            results = []
            for ref in own:
                for low in range(0, ref.shape[0], capacity):
                    results.append(ref[low : low + capacity, columns])
            total = spread(*made, results)
            total = total + own_part(near, i, capacity, same_ref, other_ref, columns)
            out_ref[:, columns] = total.astype(BF16)

    by_columns(up_ref.shape[1], piece)


def near_back_body(chips, capacity, count, place_ref, *refs):
    blocks = refs[:count]
    same_ref, other_ref = refs[count : count + 2]
    outs = refs[count + 2 :]
    near = [own_weighed(block_ref, place_ref, chips, capacity) for block_ref in blocks]

    def piece(columns):
        for i, out_ref in enumerate(outs):
            total = own_part(near[i], i, capacity, same_ref, other_ref, columns)
            out_ref[:, columns] = total.astype(BF16)

    by_columns(same_ref.shape[1], piece)


def mixer_norm_body(tokens_ref, gain_ref, _, out_ref):
    normalized(tokens_ref, gain_ref, out_ref)


def ring_of_four(me):
    return me, me + 1 - 2 * (me & 1), 3 - me, (me + 2) & 3


def mixer_first_body(place_ref, *refs):
    blocks, weight_ref, out_ref, held_ref = refs[:4], *refs[4:]
    rows = blocks[0].shape[0]
    for block_ref, place in zip(blocks, ring_of_four(place_ref[2])):
        held_ref[pl.ds(pl.multiple_of(place * rows, rows), rows), :] = block_ref[...]

    @pl.loop(0, 4)
    def _(i):
        here = pl.ds(pl.multiple_of(i * rows, rows), rows)
        made = jnp.dot(held_ref[here, :], weight_ref[...], preferred_element_type=F32)
        out_ref[here, :] = made.astype(BF16)


def mixer_second_body(
    place_ref, rim_ref, rows_ref, group_ref, scale_ref, weight_ref, out_ref, extended_ref, grouped_ref
):
    members, part = out_ref.shape[0], out_ref.shape[1]
    rim, total = rim_ref.shape[0], rows_ref.shape[0]
    rows = total // 2
    extended_ref[0:rim, :] = rim_ref[...]
    extended_ref[rim:, :] = rows_ref[...]
    window = lax.shift_left(jnp.int32(2), place_ref[2])
    behind = (
        lax.broadcasted_iota(jnp.int32, (rows, rows + rim), 0)
        - lax.broadcasted_iota(jnp.int32, (rows, rows + rim), 1)
        + rim
    )
    inside = jnp.where((behind >= 0) & (behind < window), 1.0, 0.0).astype(BF16)

    @pl.loop(0, 2)
    def _(k):
        at = pl.multiple_of(k * rows, rows)
        values = rows_ref[pl.ds(at, rows), :].astype(F32)
        sums = jnp.dot(
            inside, extended_ref[pl.ds(at, rows + rim), :], preferred_element_type=F32
        )
        position = place_ref[3] * total + at + 1 + lax.broadcasted_iota(jnp.int32, (rows, 1), 0)
        counts = jnp.minimum(position, window).astype(F32)
        pooled = (sums / counts - values).astype(BF16)
        made = jnp.dot(pooled, group_ref[...], preferred_element_type=F32)
        grouped_ref[pl.ds(at, rows), :] = (made * scale_ref[...].astype(F32)).astype(BF16)

    def piece(columns):
        made = jnp.dot(grouped_ref[...], weight_ref[:, columns], preferred_element_type=F32)
        for k in range(members):
            out_ref[k, :, columns] = made[k * part : (k + 1) * part].astype(BF16)

    by_columns(weight_ref.shape[1], piece)


def sum_body(*refs):
    planes, out_ref = [], refs[-1]
    for ref in refs[:-1]:
        planes += [ref] if len(ref.shape) == 2 else [ref.at[i] for i in range(ref.shape[0])]
    pieces = 8
    rows = out_ref.shape[0] // pieces

    @pl.loop(0, pieces)
    def _(i):
        here = pl.ds(pl.multiple_of(i * rows, rows), rows)
        total = planes[0][here, :].astype(F32)
        for ref in planes[1:]:
            total = total + ref[here, :].astype(F32)
        out_ref[here, :] = total.astype(BF16)


def whole_sum(*values):
    return call(6, sum_body, array(*values[0].shape[-2:]), *values, scalars=0)


def summed(*values):
    total = values[0].astype(F32)
    for value in values[1:]:
        total = total + value.astype(F32)
    return total.astype(BF16)


def mixer(
    place, mixer_tokens, mixer_gain, in_weight, group_weight, channel_scale, out_weight, wait
):
    rows, width = mixer_tokens.shape
    members = lax.axis_size("tp")
    columns = in_weight.shape[1]
    normed = call(
        6,
        mixer_norm_body,
        array(rows, width),
        mixer_tokens,
        mixer_gain[None],
        wait,
        scalars=0,
        waits=1,
    )
    blocks = [normed] + [exchanged(normed, "tp", phase) for phase in (0, 1)]
    blocks.append(opposite(normed, "tp"))
    pooled_in = call(
        12,
        mixer_first_body,
        array(rows * members, columns),
        place,
        *blocks,
        in_weight,
        scratch=[pltpu.VMEM((rows * members, width), BF16)],
    )
    rim = shifted(pooled_in[rows * members - WINDOW_MAX :], "ep", 1)
    parts = call(
        16,
        mixer_second_body,
        jax.ShapeDtypeStruct((members, rows, width), BF16),
        place,
        rim,
        pooled_in,
        group_weight[0],
        channel_scale[None],
        out_weight,
        scratch=[
            pltpu.VMEM((rows * members + WINDOW_MAX, columns), BF16),
            pltpu.VMEM((rows * members, columns), BF16),
        ],
    )
    parts = lax.all_to_all(parts, "tp", 0, 0, tiled=True)
    return whole_sum(parts)


def local(
    mixer_tokens,
    mixer_gain,
    in_weight,
    group_weight,
    channel_scale,
    out_weight,
    expert_tokens,
    expert_gain,
    route_ids,
    route_weights,
    gate_weight,
    up_weight,
    down_weight,
):
    rows, width = expert_tokens.shape
    chips = lax.axis_size("ep") // 2
    capacity = 4 * rows // (2 * chips)
    side = lax.axis_index("ep")
    place = jnp.stack([side // 2, side % 2, lax.axis_index("tp"), side]).astype(jnp.int32)
    block_rows = rows + META

    gates, uppers = gate_weight[0], up_weight[0]
    half = down_weight.shape[1] // 2
    gate_pair = [exchanged(gates, "tp", phase) for phase in (0, 1)]
    upper_pair = [exchanged(uppers, "tp", phase) for phase in (0, 1)]
    down_pair = [exchanged(down_weight[0], "tp", phase) for phase in (0, 1)]
    gate_last = exchanged(gate_pair[1], "tp", 0)
    upper_last = exchanged(upper_pair[0], "tp", 1)
    downs_last = [exchanged(down_pair[1][:half], "tp", 0), exchanged(down_pair[0][half:], "tp", 1)]

    block = call(
        6,
        pack_body,
        array(block_rows, width),
        route_ids.T,
        route_weights.T,
        expert_tokens,
        expert_gain[None],
        scalars=0,
    )
    ups, downs = [block], [block]
    for k in range(4):
        ups.append(exchanged(ups[-1], "ep", k % 2, 2))
        downs.append(exchanged(downs[-1], "ep", 1 - k % 2, 2))
    pieces = [array(high - low, width) for low, high in far_cuts(capacity)]
    far = call(
        8, functools.partial(relay_body, chips, capacity), pieces * 2, place, ups[4], downs[4]
    )
    far = [thrown(far[k], k + 1) for k in range(4)] + [
        thrown(far[4 + k], -(k + 1)) for k in range(4)
    ]
    blocks = [block] + ups[1:4] + downs[1:4] + [ups[4], downs[4]]
    near_same, near_other = call(
        12,
        functools.partial(near_body, chips, capacity),
        [array(9 * capacity, width)] * 2,
        place,
        *blocks,
    )
    far_same, other = call(
        6,
        functools.partial(unpack_body, capacity),
        [array(7 * capacity, width), array(16 * capacity, width)],
        near_other,
        *far,
        scalars=0,
    )
    other = swapped(other, "ep")

    parts = [far_same, near_same, other]
    sizes = [7 * capacity] * 2 + [9 * capacity] * 2
    total = sum(sizes)
    ff = gates.shape[1]
    rows_scratch = [pltpu.VMEM((total, width), BF16)]
    hidden = call(
        24,
        functools.partial(hidden_body, 3),
        array(total, 3 * ff),
        *parts,
        gates,
        uppers,
        gate_pair[0],
        upper_pair[0],
        gate_pair[1],
        upper_pair[1],
        scalars=0,
        scratch=rows_scratch,
    )
    hidden_last = call(
        16,
        functools.partial(hidden_body, 1),
        array(total, ff),
        *parts,
        gate_last,
        upper_last,
        hidden,
        scalars=0,
        waits=1,
        scratch=rows_scratch,
    )

    def results(first, sizes):
        return call(
            16,
            functools.partial(down_body, first, sizes, 2),
            [array(size, width) for size in sizes],
            hidden,
            hidden_last,
            down_weight[0],
            *down_pair,
            *downs_last,
            scalars=0,
        )

    far_same, far_other = results(0, sizes[:2])
    near_same, near_other = results(sum(sizes[:2]), sizes[2:])

    far_other = swapped(far_other, "ep")
    near_other = swapped(near_other, "ep")
    back = call(
        6, functools.partial(far_back_body, capacity), pieces * 2, far_same, far_other, scalars=0
    )
    back = [returned(back[k], k + 1) for k in range(4)] + [
        returned(back[4 + k], -(k + 1)) for k in range(4)
    ]
    kept = call(
        16,
        functools.partial(near_back_body, chips, capacity, 7),
        [array(rows, width)] * 7,
        place,
        *blocks[:7],
        near_same,
        near_other,
    )
    up_sum, down_sum = call(
        10,
        functools.partial(turn_body, chips, capacity, (7, 8)),
        [array(rows, width)] * 2,
        place,
        ups[4],
        downs[4],
        near_same,
        near_other,
        *back,
    )
    for k in (3, 2, 1, 0):
        up_sum = exchanged(up_sum, "ep", k % 2, 2)
        down_sum = exchanged(down_sum, "ep", 1 - k % 2, 2)
        if k > 0:
            up_sum = summed(up_sum, kept[k])
            down_sum = summed(down_sum, kept[3 + k])
    expert_mix = whole_sum(up_sum, down_sum, kept[0])

    mixed_tokens = mixer(
        place,
        mixer_tokens,
        mixer_gain,
        in_weight,
        group_weight,
        channel_scale,
        out_weight,
        hidden_last,
    )
    return (mixed_tokens, expert_mix)


def solution(mesh):
    placed = (
        P(("grp", "ep", "tp"), None),
        P(),
        P(None, "tp"),
        P("tp", None, None),
        P("tp"),
        P("tp", None),
        P(("grp", "ep", "tp"), None),
        P(),
        P(("grp", "ep", "tp"), None),
        P(("grp", "ep", "tp"), None),
        P("ep", None, "tp"),
        P("ep", None, "tp"),
        P("ep", "tp", None),
    )

    return jax.shard_map(
        local,
        mesh=mesh,
        in_specs=placed,
        out_specs=(P(("grp", "ep", "tp"), None), P(("grp", "ep", "tp"), None)),
        check_vma=False,
    )
```

```python
import functools

import jax
import jax.numpy as jnp
from jax import lax
from jax.experimental import pallas as pl
from jax.experimental.pallas import tpu as pltpu
from jax.sharding import PartitionSpec as P


WINDOW_MAX = 16
META = 8
F32 = jnp.float32
BF16 = jnp.bfloat16


def shifted(value, axis, by):
    devices = lax.axis_size(axis)
    pairs = [(i, i + by) for i in range(devices) if 0 <= i + by < devices]
    return lax.ppermute(value, axis, pairs)


def exchanged(value, axis, phase, width=1):
    devices = lax.axis_size(axis)
    groups = devices // width
    pairs = []
    for i in range(devices):
        group, place = divmod(i, width)
        partner = (group + (1 if group % 2 == phase else -1)) % groups
        pairs.append((i, partner * width + place))
    return lax.ppermute(value, axis, pairs)


def thrown(value, by):
    devices = lax.axis_size("ep")
    pairs = [(i, (i + (2 * by if i // 2 % 2 == 0 else -2 * by)) % devices) for i in range(devices)]
    return lax.ppermute(value, "ep", pairs)


def returned(value, by):
    return thrown(value, by if by % 2 else -by)


def opposite(value, axis):
    devices = lax.axis_size(axis)
    return lax.ppermute(value, axis, [(i, (i + devices // 2) % devices) for i in range(devices)])


def swapped(value, axis):
    devices = lax.axis_size(axis)
    return lax.ppermute(value, axis, [(i, i ^ 1) for i in range(devices)])


def call(mib, body, outs, *operands, scalars=1, waits=0, scratch=()):
    specs = (
        [pl.BlockSpec(memory_space=pltpu.SMEM)] * scalars
        + [pl.BlockSpec(memory_space=pltpu.VMEM)] * (len(operands) - scalars - waits)
        + [pl.BlockSpec(memory_space=pl.ANY)] * waits
    )
    return pl.pallas_call(
        body,
        out_shape=outs,
        in_specs=specs,
        out_specs=jax.tree.map(lambda _: pl.BlockSpec(memory_space=pltpu.VMEM), outs),
        scratch_shapes=list(scratch),
        compiler_params=pltpu.CompilerParams(vmem_limit_bytes=mib * 1024 * 1024),
    )(*operands)


def array(rows, width, dtype=BF16):
    return jax.ShapeDtypeStruct((rows, width), dtype)


def normalized(tokens_ref, gain_ref, out_ref, size=16):
    @pl.loop(0, tokens_ref.shape[0] // size)
    def _(i):
        here = pl.ds(pl.multiple_of(i * size, size), size)
        values = tokens_ref[here, :].astype(F32)
        scaled = values * lax.rsqrt(jnp.mean(values * values, axis=-1, keepdims=True) + 1e-06)
        out_ref[here, :] = (scaled * gain_ref[...].astype(F32)).astype(BF16)


def pack_body(ids_ref, weights_ref, tokens_ref, gain_ref, out_ref):
    rows, width = tokens_ref.shape
    normalized(tokens_ref, gain_ref, out_ref)
    weights = weights_ref[...]
    first, second = weights[0:1], weights[1:2]
    both = first + second
    lines = [ids_ref[0:1].astype(F32), ids_ref[1:2].astype(F32)]
    for share in (first / both, second / both):
        high = share.astype(BF16).astype(F32)
        lines += [high, share - high]
    lines += [jnp.zeros_like(first)] * (META - len(lines))
    meta = jnp.concatenate(lines, axis=0)
    meta = jnp.concatenate([meta, jnp.zeros((META, width - rows), F32)], axis=1)
    out_ref[rows:, :] = meta.astype(BF16)


def slots_of(block_ref, place_ref, chips, sign, count, capacity, kept):
    rows = block_ref.shape[0] - META
    meta = block_ref[rows:, 0:rows].astype(F32)
    chip, core = place_ref[0], place_ref[1]
    index = lax.broadcasted_iota(jnp.int32, (count, rows), 0)
    step = lax.shift_right_logical(index, 1)
    away = sign * (1 - 2 * (chip & 1))
    named = chip + away * (1 + step) + chips if sign else chip + 0 * step
    named = jnp.where(named >= chips, named - chips, named)
    named = jnp.where(named >= chips, named - chips, named)
    expert = (2 * named + ((core + (index & 1)) & 1)).astype(F32)
    is_first, is_second = meta[0:1] == expert, meta[1:2] == expert
    match = jnp.where(is_first, 1.0, 0.0) + jnp.where(is_second, 1.0, 0.0)
    shares = jnp.where(is_first, meta[2:3] + meta[3:4], 0.0) + jnp.where(
        is_second, meta[4:5] + meta[5:6], 0.0
    )
    upto = (
        lax.broadcasted_iota(jnp.int32, (rows, rows), 0)
        <= lax.broadcasted_iota(jnp.int32, (rows, rows), 1)
    ).astype(F32).astype(BF16)
    rank = jnp.dot(match.astype(BF16), upto, preferred_element_type=F32)
    slot = jnp.where(match > 0.5, rank - 1.0, -1.0)
    number = lax.broadcasted_iota(jnp.int32, (capacity, rows), 0).astype(F32)
    hot = [jnp.where(slot[e : e + 1] == number, 1.0, 0.0) for e in kept]
    return hot, [shares[e : e + 1] for e in kept]


def by_columns(width, body, pieces=8):
    @pl.loop(0, pieces)
    def _(i):
        body(pl.ds(pl.multiple_of(i * (width // pieces), 128), width // pieces))


def picked(chosen, block_ref, columns):
    rows = block_ref.shape[0] - META
    return jnp.dot(chosen, block_ref[0:rows, columns], preferred_element_type=F32).astype(BF16)


def weighed(hot, shares):
    values = [jnp.sum(h * s, axis=1, keepdims=True) for h, s in zip(hot, shares)]
    return jnp.concatenate(hot, axis=0).T.astype(BF16), values


def spread(chosen, values, results):
    scaled = [(v * r.astype(F32)).astype(BF16) for v, r in zip(values, results)]
    return jnp.dot(chosen, jnp.concatenate(scaled, axis=0), preferred_element_type=F32)


KEPT = {1: (0, 1, 2, 3, 4, 5, 6), -1: (0, 1, 2, 3, 4, 5, 7)}


def far_cuts(capacity):
    return [(2 * capacity * k, 2 * capacity * k + 2 * capacity) for k in range(3)] + [
        (6 * capacity, 7 * capacity)
    ]


def relay_body(chips, capacity, place_ref, up_ref, down_ref, *outs):
    todo = []
    for sign, block_ref, own in ((1, up_ref, outs[:4]), (-1, down_ref, outs[4:])):
        hot, _ = slots_of(block_ref, place_ref, chips, sign, 8, capacity, KEPT[sign])
        todo.append((jnp.concatenate(hot, axis=0).astype(BF16), block_ref, own))

    def piece(columns):
        for chosen, block_ref, own in todo:
            rows = picked(chosen, block_ref, columns)
            for (low, high), out_ref in zip(far_cuts(capacity), own):
                out_ref[:, columns] = rows[low:high]

    by_columns(up_ref.shape[1], piece)


def near_body(chips, capacity, place_ref, *refs):
    blocks, (same_ref, other_ref) = refs[:-2], refs[-2:]
    chosen = []
    for block_ref in blocks:
        hot, _ = slots_of(block_ref, place_ref, chips, 0, 8, capacity, (0, 1))
        chosen.append(jnp.concatenate(hot, axis=0).astype(BF16))

    def piece(columns):
        for i, block_ref in enumerate(blocks):
            rows = picked(chosen[i], block_ref, columns)
            same_ref[i * capacity : (i + 1) * capacity, columns] = rows[:capacity]
            other_ref[i * capacity : (i + 1) * capacity, columns] = rows[capacity:]

    by_columns(same_ref.shape[1], piece)


def unpack_body(capacity, near_ref, *refs):
    far, (same_ref, other_ref) = refs[:-2], refs[-2:]
    low = near_ref.shape[0]
    other_ref[0:low, :] = near_ref[...]
    for i in range(7):
        here = slice(i * capacity, (i + 1) * capacity)
        same_ref[here, :] = far[i][0:capacity, :]
    for i, k in enumerate((0, 1, 2, 4, 5, 6)):
        at = low + i * capacity
        other_ref[at : at + capacity, :] = far[k][capacity : 2 * capacity, :]
    other_ref[low + 6 * capacity :, :] = far[7][...]


def hidden_body(pairs, far_same, near_same, other, *refs):
    weights, out_ref, rows_ref = refs[: 2 * pairs], refs[-2], refs[-1]
    near, far = near_same.shape[0], far_same.shape[0]
    rows_ref[0:far, :] = far_same[...]
    rows_ref[far : 2 * far, :] = other[near:, :]
    rows_ref[2 * far : 2 * far + near, :] = near_same[...]
    rows_ref[2 * far + near :, :] = other[0:near, :]
    low = rows_ref.shape[0]

    @pl.loop(0, 4)
    def _(i):
        here = pl.ds(pl.multiple_of(i * (low // 4), 128), low // 4)
        for k in range(pairs):
            gate = jnp.dot(rows_ref[here, :], weights[2 * k][...], preferred_element_type=F32)
            upper = jnp.dot(rows_ref[here, :], weights[2 * k + 1][...], preferred_element_type=F32)
            made = (gate / (1.0 + jnp.exp(-gate)) * upper).astype(BF16)
            columns = made.shape[1]
            out_ref[here, k * columns : (k + 1) * columns] = made


def down_body(first, sizes, count, *refs):
    rows = sum(sizes)
    hidden = jnp.concatenate([ref[first : first + rows, :] for ref in refs[:count]], axis=1)
    outs = refs[len(refs) - len(sizes) :]
    weights = refs[count : len(refs) - len(sizes)]

    def piece(columns):
        total, low = 0.0, 0
        for ref in weights:
            total = total + jnp.dot(
                hidden[:, low : low + ref.shape[0]], ref[:, columns], preferred_element_type=F32
            )
            low += ref.shape[0]
        at = 0
        for size, out_ref in zip(sizes, outs):
            out_ref[:, columns] = total[at : at + size].astype(BF16)
            at += size

    by_columns(outs[0].shape[1], piece)


def far_back_body(capacity, same_ref, other_ref, *outs):
    for i in range(3):
        for base, own in ((0, outs[:4]), (4, outs[4:])):
            j = i + base
            k = i if base == 0 else i + 3
            own[i][0:capacity, :] = same_ref[j * capacity : (j + 1) * capacity, :]
            own[i][capacity:, :] = other_ref[k * capacity : (k + 1) * capacity, :]
    outs[3][...] = same_ref[3 * capacity : 4 * capacity, :]
    outs[7][...] = other_ref[6 * capacity : 7 * capacity, :]


def own_weighed(block_ref, place_ref, chips, capacity):
    return weighed(*slots_of(block_ref, place_ref, chips, 0, 8, capacity, (0, 1)))


def own_part(made, i, capacity, same_ref, other_ref, columns):
    low, high = i * capacity, (i + 1) * capacity
    return spread(*made, [same_ref[low:high, columns], other_ref[low:high, columns]])


def turn_body(chips, capacity, at, place_ref, up_ref, down_ref, same_ref, other_ref, *refs):
    far, outs = refs[:8], refs[8:]
    todo = []
    for sign, block_ref, own, i, out_ref in (
        (1, up_ref, far[:4], at[0], outs[0]),
        (-1, down_ref, far[4:], at[1], outs[1]),
    ):
        made = weighed(*slots_of(block_ref, place_ref, chips, sign, 8, capacity, KEPT[sign]))
        near = own_weighed(block_ref, place_ref, chips, capacity)
        todo.append((made, near, own, i, out_ref))

    def piece(columns):
        for made, near, own, i, out_ref in todo:
            results = []
            for ref in own:
                for low in range(0, ref.shape[0], capacity):
                    results.append(ref[low : low + capacity, columns])
            total = spread(*made, results)
            total = total + own_part(near, i, capacity, same_ref, other_ref, columns)
            out_ref[:, columns] = total.astype(BF16)

    by_columns(up_ref.shape[1], piece)


def near_back_body(chips, capacity, count, place_ref, *refs):
    blocks = refs[:count]
    same_ref, other_ref = refs[count : count + 2]
    outs = refs[count + 2 :]
    near = [own_weighed(block_ref, place_ref, chips, capacity) for block_ref in blocks]

    def piece(columns):
        for i, out_ref in enumerate(outs):
            total = own_part(near[i], i, capacity, same_ref, other_ref, columns)
            out_ref[:, columns] = total.astype(BF16)

    by_columns(same_ref.shape[1], piece)


def mixer_norm_body(tokens_ref, gain_ref, _, out_ref):
    normalized(tokens_ref, gain_ref, out_ref)


def ring_of_four(me):
    return me, me + 1 - 2 * (me & 1), 3 - me, (me + 2) & 3


def mixer_first_body(place_ref, *refs):
    blocks, weight_ref, out_ref, held_ref = refs[:4], *refs[4:]
    rows = blocks[0].shape[0]
    for block_ref, place in zip(blocks, ring_of_four(place_ref[2])):
        held_ref[pl.ds(pl.multiple_of(place * rows, rows), rows), :] = block_ref[...]

    @pl.loop(0, 4)
    def _(i):
        here = pl.ds(pl.multiple_of(i * rows, rows), rows)
        made = jnp.dot(held_ref[here, :], weight_ref[...], preferred_element_type=F32)
        out_ref[here, :] = made.astype(BF16)


def mixer_second_body(
    place_ref, rim_ref, rows_ref, group_ref, scale_ref, weight_ref, out_ref, extended_ref, grouped_ref
):
    members, part = out_ref.shape[0], out_ref.shape[1]
    rim, total = rim_ref.shape[0], rows_ref.shape[0]
    rows = part
    extended_ref[0:rim, :] = rim_ref[...]
    extended_ref[rim:, :] = rows_ref[...]
    window = lax.shift_left(jnp.int32(2), place_ref[2])
    behind = (
        lax.broadcasted_iota(jnp.int32, (rows, rows + rim), 0)
        - lax.broadcasted_iota(jnp.int32, (rows, rows + rim), 1)
        + rim
    )
    inside = jnp.where((behind >= 0) & (behind < window), 1.0, 0.0).astype(BF16)
    for at in range(0, total, rows):
        values = rows_ref[at : at + rows, :].astype(F32)
        sums = jnp.dot(inside, extended_ref[at : at + rows + rim, :], preferred_element_type=F32)
        position = place_ref[3] * total + at + 1 + lax.broadcasted_iota(jnp.int32, (rows, 1), 0)
        counts = jnp.minimum(position, window).astype(F32)
        pooled = (sums / counts - values).astype(BF16)
        made = jnp.dot(pooled, group_ref[...], preferred_element_type=F32)
        grouped_ref[at : at + rows, :] = (made * scale_ref[...].astype(F32)).astype(BF16)

    def piece(columns):
        made = jnp.dot(grouped_ref[...], weight_ref[:, columns], preferred_element_type=F32)
        for k in range(members):
            out_ref[k, :, columns] = made[k * part : (k + 1) * part].astype(BF16)

    by_columns(weight_ref.shape[1], piece)


def sum_body(*refs):
    planes, out_ref = [], refs[-1]
    for ref in refs[:-1]:
        planes += [ref] if len(ref.shape) == 2 else [ref.at[i] for i in range(ref.shape[0])]
    pieces = 8
    rows = out_ref.shape[0] // pieces

    @pl.loop(0, pieces)
    def _(i):
        here = pl.ds(pl.multiple_of(i * rows, rows), rows)
        total = planes[0][here, :].astype(F32)
        for ref in planes[1:]:
            total = total + ref[here, :].astype(F32)
        out_ref[here, :] = total.astype(BF16)


def whole_sum(*values):
    return call(6, sum_body, array(*values[0].shape[-2:]), *values, scalars=0)


def summed(*values):
    total = values[0].astype(F32)
    for value in values[1:]:
        total = total + value.astype(F32)
    return total.astype(BF16)


def mixer(
    place, mixer_tokens, mixer_gain, in_weight, group_weight, channel_scale, out_weight, wait
):
    rows, width = mixer_tokens.shape
    members = lax.axis_size("tp")
    columns = in_weight.shape[1]
    normed = call(
        6,
        mixer_norm_body,
        array(rows, width),
        mixer_tokens,
        mixer_gain[None],
        wait,
        scalars=0,
        waits=1,
    )
    blocks = [normed] + [exchanged(normed, "tp", phase) for phase in (0, 1)]
    blocks.append(opposite(normed, "tp"))
    pooled_in = call(
        12,
        mixer_first_body,
        array(rows * members, columns),
        place,
        *blocks,
        in_weight,
        scratch=[pltpu.VMEM((rows * members, width), BF16)],
    )
    rim = shifted(pooled_in[rows * members - WINDOW_MAX :], "ep", 1)
    parts = call(
        16,
        mixer_second_body,
        jax.ShapeDtypeStruct((members, rows, width), BF16),
        place,
        rim,
        pooled_in,
        group_weight[0],
        channel_scale[None],
        out_weight,
        scratch=[
            pltpu.VMEM((rows * members + WINDOW_MAX, columns), BF16),
            pltpu.VMEM((rows * members, columns), BF16),
        ],
    )
    parts = lax.all_to_all(parts, "tp", 0, 0, tiled=True)
    return whole_sum(parts)


def local(
    mixer_tokens,
    mixer_gain,
    in_weight,
    group_weight,
    channel_scale,
    out_weight,
    expert_tokens,
    expert_gain,
    route_ids,
    route_weights,
    gate_weight,
    up_weight,
    down_weight,
):
    rows, width = expert_tokens.shape
    chips = lax.axis_size("ep") // 2
    capacity = 4 * rows // (2 * chips)
    side = lax.axis_index("ep")
    place = jnp.stack([side // 2, side % 2, lax.axis_index("tp"), side]).astype(jnp.int32)
    block_rows = rows + META

    gates, uppers = gate_weight[0], up_weight[0]
    half = down_weight.shape[1] // 2
    gate_pair = [exchanged(gates, "tp", phase) for phase in (0, 1)]
    upper_pair = [exchanged(uppers, "tp", phase) for phase in (0, 1)]
    down_pair = [exchanged(down_weight[0], "tp", phase) for phase in (0, 1)]
    gate_last = exchanged(gate_pair[1], "tp", 0)
    upper_last = exchanged(upper_pair[0], "tp", 1)
    downs_last = [exchanged(down_pair[1][:half], "tp", 0), exchanged(down_pair[0][half:], "tp", 1)]

    block = call(
        6,
        pack_body,
        array(block_rows, width),
        route_ids.T,
        route_weights.T,
        expert_tokens,
        expert_gain[None],
        scalars=0,
    )
    ups, downs = [block], [block]
    for k in range(4):
        ups.append(exchanged(ups[-1], "ep", k % 2, 2))
        downs.append(exchanged(downs[-1], "ep", 1 - k % 2, 2))
    pieces = [array(high - low, width) for low, high in far_cuts(capacity)]
    far = call(
        8, functools.partial(relay_body, chips, capacity), pieces * 2, place, ups[4], downs[4]
    )
    far = [thrown(far[k], k + 1) for k in range(4)] + [
        thrown(far[4 + k], -(k + 1)) for k in range(4)
    ]
    blocks = [block] + ups[1:4] + downs[1:4] + [ups[4], downs[4]]
    near_same, near_other = call(
        12,
        functools.partial(near_body, chips, capacity),
        [array(9 * capacity, width)] * 2,
        place,
        *blocks,
    )
    far_same, other = call(
        6,
        functools.partial(unpack_body, capacity),
        [array(7 * capacity, width), array(16 * capacity, width)],
        near_other,
        *far,
        scalars=0,
    )
    other = swapped(other, "ep")

    parts = [far_same, near_same, other]
    sizes = [7 * capacity] * 2 + [9 * capacity] * 2
    total = sum(sizes)
    ff = gates.shape[1]
    rows_scratch = [pltpu.VMEM((total, width), BF16)]
    hidden = call(
        24,
        functools.partial(hidden_body, 3),
        array(total, 3 * ff),
        *parts,
        gates,
        uppers,
        gate_pair[0],
        upper_pair[0],
        gate_pair[1],
        upper_pair[1],
        scalars=0,
        scratch=rows_scratch,
    )
    hidden_last = call(
        16,
        functools.partial(hidden_body, 1),
        array(total, ff),
        *parts,
        gate_last,
        upper_last,
        hidden,
        scalars=0,
        waits=1,
        scratch=rows_scratch,
    )

    def results(first, sizes):
        return call(
            16,
            functools.partial(down_body, first, sizes, 2),
            [array(size, width) for size in sizes],
            hidden,
            hidden_last,
            down_weight[0],
            *down_pair,
            *downs_last,
            scalars=0,
        )

    far_same, far_other = results(0, sizes[:2])
    near_same, near_other = results(sum(sizes[:2]), sizes[2:])

    far_other = swapped(far_other, "ep")
    near_other = swapped(near_other, "ep")
    back = call(
        6, functools.partial(far_back_body, capacity), pieces * 2, far_same, far_other, scalars=0
    )
    back = [returned(back[k], k + 1) for k in range(4)] + [
        returned(back[4 + k], -(k + 1)) for k in range(4)
    ]
    kept = call(
        16,
        functools.partial(near_back_body, chips, capacity, 7),
        [array(rows, width)] * 7,
        place,
        *blocks[:7],
        near_same,
        near_other,
    )
    up_sum, down_sum = call(
        10,
        functools.partial(turn_body, chips, capacity, (7, 8)),
        [array(rows, width)] * 2,
        place,
        ups[4],
        downs[4],
        near_same,
        near_other,
        *back,
    )
    for k in (3, 2, 1, 0):
        up_sum = exchanged(up_sum, "ep", k % 2, 2)
        down_sum = exchanged(down_sum, "ep", 1 - k % 2, 2)
        if k > 0:
            up_sum = summed(up_sum, kept[k])
            down_sum = summed(down_sum, kept[3 + k])
    expert_mix = summed(up_sum, down_sum, kept[0])

    mixed_tokens = mixer(
        place,
        mixer_tokens,
        mixer_gain,
        in_weight,
        group_weight,
        channel_scale,
        out_weight,
        hidden_last,
    )
    return (mixed_tokens, expert_mix)


def solution(mesh):
    placed = (
        P(("grp", "ep", "tp"), None),
        P(),
        P(None, "tp"),
        P("tp", None, None),
        P("tp"),
        P("tp", None),
        P(("grp", "ep", "tp"), None),
        P(),
        P(("grp", "ep", "tp"), None),
        P(("grp", "ep", "tp"), None),
        P("ep", None, "tp"),
        P("ep", None, "tp"),
        P("ep", "tp", None),
    )

    return jax.shard_map(
        local,
        mesh=mesh,
        in_specs=placed,
        out_specs=(P(("grp", "ep", "tp"), None), P(("grp", "ep", "tp"), None)),
        check_vma=False,
    )
```

```python
import functools

import jax
import jax.numpy as jnp
from jax import lax
from jax.experimental import pallas as pl
from jax.experimental.pallas import tpu as pltpu
from jax.sharding import PartitionSpec as P


WINDOW_MAX = 16
META = 8
F32 = jnp.float32
BF16 = jnp.bfloat16


def shifted(value, axis, by):
    devices = lax.axis_size(axis)
    pairs = [(i, i + by) for i in range(devices) if 0 <= i + by < devices]
    return lax.ppermute(value, axis, pairs)


def exchanged(value, axis, phase, width=1):
    devices = lax.axis_size(axis)
    groups = devices // width
    pairs = []
    for i in range(devices):
        group, place = divmod(i, width)
        partner = (group + (1 if group % 2 == phase else -1)) % groups
        pairs.append((i, partner * width + place))
    return lax.ppermute(value, axis, pairs)


def exchanged_by_core(value, phase):
    sides, devices = lax.axis_size("ep"), lax.axis_size("tp")
    pairs = []
    for i in range(sides * devices):
        side, place = divmod(i, devices)
        partner = (place + (1 if place % 2 == (phase + side) % 2 else -1)) % devices
        pairs.append((i, side * devices + partner))
    return lax.ppermute(value, ("ep", "tp"), pairs)


def thrown(value, by):
    devices = lax.axis_size("ep")
    pairs = [(i, (i + (2 * by if i // 2 % 2 == 0 else -2 * by)) % devices) for i in range(devices)]
    return lax.ppermute(value, "ep", pairs)


def returned(value, by):
    return thrown(value, by if by % 2 else -by)


def opposite(value, axis):
    devices = lax.axis_size(axis)
    return lax.ppermute(value, axis, [(i, (i + devices // 2) % devices) for i in range(devices)])


def swapped(value, axis):
    devices = lax.axis_size(axis)
    return lax.ppermute(value, axis, [(i, i ^ 1) for i in range(devices)])


def call(mib, body, outs, *operands, scalars=1, waits=0, scratch=()):
    specs = (
        [pl.BlockSpec(memory_space=pltpu.SMEM)] * scalars
        + [pl.BlockSpec(memory_space=pltpu.VMEM)] * (len(operands) - scalars - waits)
        + [pl.BlockSpec(memory_space=pl.ANY)] * waits
    )
    return pl.pallas_call(
        body,
        out_shape=outs,
        in_specs=specs,
        out_specs=jax.tree.map(lambda _: pl.BlockSpec(memory_space=pltpu.VMEM), outs),
        scratch_shapes=list(scratch),
        compiler_params=pltpu.CompilerParams(vmem_limit_bytes=mib * 1024 * 1024),
    )(*operands)


def array(rows, width, dtype=BF16):
    return jax.ShapeDtypeStruct((rows, width), dtype)


def normalized(tokens_ref, gain_ref, out_ref, size=16):
    @pl.loop(0, tokens_ref.shape[0] // size)
    def _(i):
        here = pl.ds(pl.multiple_of(i * size, size), size)
        values = tokens_ref[here, :].astype(F32)
        scaled = values * lax.rsqrt(jnp.mean(values * values, axis=-1, keepdims=True) + 1e-06)
        out_ref[here, :] = (scaled * gain_ref[...].astype(F32)).astype(BF16)


def pack_body(ids_ref, weights_ref, tokens_ref, gain_ref, out_ref):
    rows, width = tokens_ref.shape
    normalized(tokens_ref, gain_ref, out_ref)
    weights = weights_ref[...]
    first, second = weights[0:1], weights[1:2]
    both = first + second
    lines = [ids_ref[0:1].astype(F32), ids_ref[1:2].astype(F32)]
    for share in (first / both, second / both):
        high = share.astype(BF16).astype(F32)
        lines += [high, share - high]
    lines += [jnp.zeros_like(first)] * (META - len(lines))
    meta = jnp.concatenate(lines, axis=0)
    meta = jnp.concatenate([meta, jnp.zeros((META, width - rows), F32)], axis=1)
    out_ref[rows:, :] = meta.astype(BF16)


def slots_of(block_ref, place_ref, chips, sign, count, capacity, kept):
    rows = block_ref.shape[0] - META
    meta = block_ref[rows:, 0:rows].astype(F32)
    chip, core = place_ref[0], place_ref[1]
    index = lax.broadcasted_iota(jnp.int32, (count, rows), 0)
    step = lax.shift_right_logical(index, 1)
    away = sign * (1 - 2 * (chip & 1))
    named = chip + away * (1 + step) + chips if sign else chip + 0 * step
    named = jnp.where(named >= chips, named - chips, named)
    named = jnp.where(named >= chips, named - chips, named)
    expert = (2 * named + ((core + (index & 1)) & 1)).astype(F32)
    is_first, is_second = meta[0:1] == expert, meta[1:2] == expert
    match = jnp.where(is_first, 1.0, 0.0) + jnp.where(is_second, 1.0, 0.0)
    shares = jnp.where(is_first, meta[2:3] + meta[3:4], 0.0) + jnp.where(
        is_second, meta[4:5] + meta[5:6], 0.0
    )
    upto = (
        lax.broadcasted_iota(jnp.int32, (rows, rows), 0)
        <= lax.broadcasted_iota(jnp.int32, (rows, rows), 1)
    ).astype(F32).astype(BF16)
    rank = jnp.dot(match.astype(BF16), upto, preferred_element_type=F32)
    slot = jnp.where(match > 0.5, rank - 1.0, -1.0)
    number = lax.broadcasted_iota(jnp.int32, (capacity, rows), 0).astype(F32)
    hot = [jnp.where(slot[e : e + 1] == number, 1.0, 0.0) for e in kept]
    return hot, [shares[e : e + 1] for e in kept]


def by_columns(width, body, pieces=8):
    @pl.loop(0, pieces)
    def _(i):
        body(pl.ds(pl.multiple_of(i * (width // pieces), 128), width // pieces))


def picked(chosen, block_ref, columns):
    rows = block_ref.shape[0] - META
    return jnp.dot(chosen, block_ref[0:rows, columns], preferred_element_type=F32).astype(BF16)


def weighed(hot, shares):
    values = [jnp.sum(h * s, axis=1, keepdims=True) for h, s in zip(hot, shares)]
    return jnp.concatenate(hot, axis=0).T.astype(BF16), values


def spread(chosen, values, results):
    scaled = [(v * r.astype(F32)).astype(BF16) for v, r in zip(values, results)]
    return jnp.dot(chosen, jnp.concatenate(scaled, axis=0), preferred_element_type=F32)


KEPT = {1: (0, 1, 2, 3, 4, 5, 6), -1: (0, 1, 2, 3, 4, 5, 7)}


def far_cuts(capacity):
    return [(2 * capacity * k, 2 * capacity * k + 2 * capacity) for k in range(3)] + [
        (6 * capacity, 7 * capacity)
    ]


def relay_body(chips, capacity, place_ref, up_ref, down_ref, *outs):
    todo = []
    for sign, block_ref, own in ((1, up_ref, outs[:4]), (-1, down_ref, outs[4:])):
        hot, _ = slots_of(block_ref, place_ref, chips, sign, 8, capacity, KEPT[sign])
        todo.append((jnp.concatenate(hot, axis=0).astype(BF16), block_ref, own))

    def piece(columns):
        for chosen, block_ref, own in todo:
            rows = picked(chosen, block_ref, columns)
            for (low, high), out_ref in zip(far_cuts(capacity), own):
                out_ref[:, columns] = rows[low:high]

    by_columns(up_ref.shape[1], piece)


def near_body(chips, capacity, place_ref, *refs):
    blocks, (same_ref, other_ref) = refs[:-2], refs[-2:]
    chosen = []
    for block_ref in blocks:
        hot, _ = slots_of(block_ref, place_ref, chips, 0, 8, capacity, (0, 1))
        chosen.append(jnp.concatenate(hot, axis=0).astype(BF16))

    def piece(columns):
        for i, block_ref in enumerate(blocks):
            rows = picked(chosen[i], block_ref, columns)
            same_ref[i * capacity : (i + 1) * capacity, columns] = rows[:capacity]
            other_ref[i * capacity : (i + 1) * capacity, columns] = rows[capacity:]

    by_columns(same_ref.shape[1], piece)


def unpack_body(capacity, near_ref, *refs):
    far, (same_ref, other_ref) = refs[:-2], refs[-2:]
    low = near_ref.shape[0]
    other_ref[0:low, :] = near_ref[...]
    for i in range(7):
        here = slice(i * capacity, (i + 1) * capacity)
        same_ref[here, :] = far[i][0:capacity, :]
    for i, k in enumerate((0, 1, 2, 4, 5, 6)):
        at = low + i * capacity
        other_ref[at : at + capacity, :] = far[k][capacity : 2 * capacity, :]
    other_ref[low + 6 * capacity :, :] = far[7][...]


def hidden_body(pairs, far_same, near_same, other, *refs):
    weights, out_ref, rows_ref = refs[: 2 * pairs], refs[-2], refs[-1]
    near, far = near_same.shape[0], far_same.shape[0]
    rows_ref[0:far, :] = far_same[...]
    rows_ref[far : 2 * far, :] = other[near:, :]
    rows_ref[2 * far : 2 * far + near, :] = near_same[...]
    rows_ref[2 * far + near :, :] = other[0:near, :]
    low = rows_ref.shape[0]

    @pl.loop(0, 4)
    def _(i):
        here = pl.ds(pl.multiple_of(i * (low // 4), 128), low // 4)
        for k in range(pairs):
            gate = jnp.dot(rows_ref[here, :], weights[2 * k][...], preferred_element_type=F32)
            upper = jnp.dot(rows_ref[here, :], weights[2 * k + 1][...], preferred_element_type=F32)
            made = (gate / (1.0 + jnp.exp(-gate)) * upper).astype(BF16)
            columns = made.shape[1]
            out_ref[here, k * columns : (k + 1) * columns] = made


def down_body(first, sizes, count, *refs):
    rows = sum(sizes)
    hidden = jnp.concatenate([ref[first : first + rows, :] for ref in refs[:count]], axis=1)
    outs = refs[len(refs) - len(sizes) :]
    weights = refs[count : len(refs) - len(sizes)]

    def piece(columns):
        total, low = 0.0, 0
        for ref in weights:
            total = total + jnp.dot(
                hidden[:, low : low + ref.shape[0]], ref[:, columns], preferred_element_type=F32
            )
            low += ref.shape[0]
        at = 0
        for size, out_ref in zip(sizes, outs):
            out_ref[:, columns] = total[at : at + size].astype(BF16)
            at += size

    by_columns(outs[0].shape[1], piece)


def far_back_body(capacity, same_ref, other_ref, *outs):
    for i in range(3):
        for base, own in ((0, outs[:4]), (4, outs[4:])):
            j = i + base
            k = i if base == 0 else i + 3
            own[i][0:capacity, :] = same_ref[j * capacity : (j + 1) * capacity, :]
            own[i][capacity:, :] = other_ref[k * capacity : (k + 1) * capacity, :]
    outs[3][...] = same_ref[3 * capacity : 4 * capacity, :]
    outs[7][...] = other_ref[6 * capacity : 7 * capacity, :]


def own_weighed(block_ref, place_ref, chips, capacity):
    return weighed(*slots_of(block_ref, place_ref, chips, 0, 8, capacity, (0, 1)))


def own_part(made, i, capacity, same_ref, other_ref, columns):
    low, high = i * capacity, (i + 1) * capacity
    return spread(*made, [same_ref[low:high, columns], other_ref[low:high, columns]])


def turn_body(chips, capacity, at, place_ref, up_ref, down_ref, same_ref, other_ref, *refs):
    far, outs = refs[:8], refs[8:]
    todo = []
    for sign, block_ref, own, i, out_ref in (
        (1, up_ref, far[:4], at[0], outs[0]),
        (-1, down_ref, far[4:], at[1], outs[1]),
    ):
        made = weighed(*slots_of(block_ref, place_ref, chips, sign, 8, capacity, KEPT[sign]))
        near = own_weighed(block_ref, place_ref, chips, capacity)
        todo.append((made, near, own, i, out_ref))

    def piece(columns):
        for made, near, own, i, out_ref in todo:
            results = []
            for ref in own:
                for low in range(0, ref.shape[0], capacity):
                    results.append(ref[low : low + capacity, columns])
            total = spread(*made, results)
            total = total + own_part(near, i, capacity, same_ref, other_ref, columns)
            out_ref[:, columns] = total.astype(BF16)

    by_columns(up_ref.shape[1], piece)


def near_back_body(chips, capacity, count, place_ref, *refs):
    blocks = refs[:count]
    same_ref, other_ref = refs[count : count + 2]
    outs = refs[count + 2 :]
    near = [own_weighed(block_ref, place_ref, chips, capacity) for block_ref in blocks]

    def piece(columns):
        for i, out_ref in enumerate(outs):
            total = own_part(near[i], i, capacity, same_ref, other_ref, columns)
            out_ref[:, columns] = total.astype(BF16)

    by_columns(same_ref.shape[1], piece)


def mixer_norm_body(tokens_ref, gain_ref, _, out_ref):
    normalized(tokens_ref, gain_ref, out_ref)


def ring_of_four(me):
    return me, me + 1 - 2 * (me & 1), 3 - me, (me + 2) & 3


def mixer_first_body(place_ref, *refs):
    blocks, weight_ref, out_ref, held_ref = refs[:4], *refs[4:]
    rows = blocks[0].shape[0]
    for block_ref, place in zip(blocks, ring_of_four(place_ref[2])):
        held_ref[pl.ds(pl.multiple_of(place * rows, rows), rows), :] = block_ref[...]

    @pl.loop(0, 4)
    def _(i):
        here = pl.ds(pl.multiple_of(i * rows, rows), rows)
        made = jnp.dot(held_ref[here, :], weight_ref[...], preferred_element_type=F32)
        out_ref[here, :] = made.astype(BF16)


def mixer_second_body(place_ref, rim_ref, rows_ref, group_ref, scale_ref, weight_ref, *refs):
    outs, extended_ref = refs[:4], refs[4]
    rim, total = rim_ref.shape[0], rows_ref.shape[0]
    rows = total // 4
    extended_ref[0:rim, :] = rim_ref[...]
    extended_ref[rim:, :] = rows_ref[...]
    window = lax.shift_left(jnp.int32(2), place_ref[2])
    behind = (
        lax.broadcasted_iota(jnp.int32, (rows, rows + rim), 0)
        - lax.broadcasted_iota(jnp.int32, (rows, rows + rim), 1)
        + rim
    )
    inside = jnp.where((behind >= 0) & (behind < window), 1.0, 0.0).astype(BF16)
    grouped = []
    for place in ring_of_four(place_ref[2]):
        at = pl.multiple_of(place * rows, rows)
        values = rows_ref[pl.ds(at, rows), :].astype(F32)
        sums = jnp.dot(
            inside, extended_ref[pl.ds(at, rows + rim), :], preferred_element_type=F32
        )
        position = place_ref[3] * total + at + 1 + lax.broadcasted_iota(jnp.int32, (rows, 1), 0)
        counts = jnp.minimum(position, window).astype(F32)
        pooled = (sums / counts - values).astype(BF16)
        made = jnp.dot(pooled, group_ref[...], preferred_element_type=F32)
        grouped.append((made * scale_ref[...].astype(F32)).astype(BF16))
    grouped = jnp.concatenate(grouped, axis=0)

    def piece(columns):
        made = jnp.dot(grouped, weight_ref[:, columns], preferred_element_type=F32).astype(BF16)
        for k, out_ref in enumerate(outs):
            out_ref[:, columns] = made[k * rows : (k + 1) * rows]

    by_columns(weight_ref.shape[1], piece)


def sum_body(*refs):
    planes, out_ref = [], refs[-1]
    for ref in refs[:-1]:
        planes += [ref] if len(ref.shape) == 2 else [ref.at[i] for i in range(ref.shape[0])]
    pieces = 8
    rows = out_ref.shape[0] // pieces

    @pl.loop(0, pieces)
    def _(i):
        here = pl.ds(pl.multiple_of(i * rows, rows), rows)
        total = planes[0][here, :].astype(F32)
        for ref in planes[1:]:
            total = total + ref[here, :].astype(F32)
        out_ref[here, :] = total.astype(BF16)


def whole_sum(*values):
    return call(6, sum_body, array(*values[0].shape[-2:]), *values, scalars=0)


def around(here, first, second, across):
    return [here, exchanged(first, "tp", 0), exchanged(second, "tp", 1), opposite(across, "tp")]


def mixer(
    place, mixer_tokens, mixer_gain, in_weight, group_weight, channel_scale, out_weight, wait
):
    rows, width = mixer_tokens.shape
    members = lax.axis_size("tp")
    columns = in_weight.shape[1]
    normed = call(
        6,
        mixer_norm_body,
        array(rows, width),
        mixer_tokens,
        mixer_gain[None],
        wait,
        scalars=0,
        waits=1,
    )
    blocks = around(normed, normed, normed, normed)
    pooled_in = call(
        12,
        mixer_first_body,
        array(rows * members, columns),
        place,
        *blocks,
        in_weight,
        scratch=[pltpu.VMEM((rows * members, width), BF16)],
    )
    rim = shifted(pooled_in[rows * members - WINDOW_MAX :], "ep", 1)
    parts = call(
        16,
        mixer_second_body,
        [array(rows, width)] * members,
        place,
        rim,
        pooled_in,
        group_weight[0],
        channel_scale[None],
        out_weight,
        scratch=[pltpu.VMEM((rows * members + WINDOW_MAX, columns), BF16)],
    )
    parts = around(*parts)
    return whole_sum(*parts)


def local(
    mixer_tokens,
    mixer_gain,
    in_weight,
    group_weight,
    channel_scale,
    out_weight,
    expert_tokens,
    expert_gain,
    route_ids,
    route_weights,
    gate_weight,
    up_weight,
    down_weight,
):
    rows, width = expert_tokens.shape
    chips = lax.axis_size("ep") // 2
    capacity = 4 * rows // (2 * chips)
    side = lax.axis_index("ep")
    place = jnp.stack([side // 2, side % 2, lax.axis_index("tp"), side]).astype(jnp.int32)
    block_rows = rows + META

    gates, uppers = gate_weight[0], up_weight[0]
    gate_pair = [exchanged_by_core(gates, phase) for phase in (0, 1)]
    upper_pair = [exchanged_by_core(uppers, phase) for phase in (0, 1)]
    down_pair = [exchanged_by_core(down_weight[0], phase) for phase in (0, 1)]
    gate_last = exchanged_by_core(gate_pair[1], 0)
    upper_last = exchanged_by_core(upper_pair[0], 1)
    down_last = exchanged_by_core(down_pair[1], 0)

    block = call(
        6,
        pack_body,
        array(block_rows, width),
        route_ids.T,
        route_weights.T,
        expert_tokens,
        expert_gain[None],
        scalars=0,
    )
    ups, downs = [block], [block]
    for k in range(4):
        ups.append(exchanged(ups[-1], "ep", k % 2, 2))
        downs.append(exchanged(downs[-1], "ep", 1 - k % 2, 2))
    pieces = [array(high - low, width) for low, high in far_cuts(capacity)]
    far = call(
        8, functools.partial(relay_body, chips, capacity), pieces * 2, place, ups[4], downs[4]
    )
    far = [thrown(far[k], k + 1) for k in range(4)] + [
        thrown(far[4 + k], -(k + 1)) for k in range(4)
    ]
    blocks = [block] + ups[1:4] + downs[1:4] + [ups[4], downs[4]]
    near_same, near_other = call(
        12,
        functools.partial(near_body, chips, capacity),
        [array(9 * capacity, width)] * 2,
        place,
        *blocks,
    )
    far_same, other = call(
        6,
        functools.partial(unpack_body, capacity),
        [array(7 * capacity, width), array(16 * capacity, width)],
        near_other,
        *far,
        scalars=0,
    )
    other = swapped(other, "ep")

    parts = [far_same, near_same, other]
    sizes = [7 * capacity] * 2 + [9 * capacity] * 2
    total = sum(sizes)
    ff = gates.shape[1]
    rows_scratch = [pltpu.VMEM((total, width), BF16)]
    hidden = call(
        24,
        functools.partial(hidden_body, 3),
        array(total, 3 * ff),
        *parts,
        gates,
        uppers,
        gate_pair[0],
        upper_pair[0],
        gate_pair[1],
        upper_pair[1],
        scalars=0,
        scratch=rows_scratch,
    )
    hidden_last = call(
        16,
        functools.partial(hidden_body, 1),
        array(total, ff),
        *parts,
        gate_last,
        upper_last,
        hidden,
        scalars=0,
        waits=1,
        scratch=rows_scratch,
    )

    def results(first, sizes):
        return call(
            16,
            functools.partial(down_body, first, sizes, 2),
            [array(size, width) for size in sizes],
            hidden,
            hidden_last,
            down_weight[0],
            *down_pair,
            down_last,
            scalars=0,
        )

    far_same, far_other = results(0, sizes[:2])
    near_same, near_other = results(sum(sizes[:2]), sizes[2:])

    far_other = swapped(far_other, "ep")
    near_other = swapped(near_other, "ep")
    back = call(
        6, functools.partial(far_back_body, capacity), pieces * 2, far_same, far_other, scalars=0
    )
    back = [returned(back[k], k + 1) for k in range(4)] + [
        returned(back[4 + k], -(k + 1)) for k in range(4)
    ]
    kept = call(
        16,
        functools.partial(near_back_body, chips, capacity, 7),
        [array(rows, width)] * 7,
        place,
        *blocks[:7],
        near_same,
        near_other,
    )
    up_sum, down_sum = call(
        10,
        functools.partial(turn_body, chips, capacity, (7, 8)),
        [array(rows, width)] * 2,
        place,
        ups[4],
        downs[4],
        near_same,
        near_other,
        *back,
    )
    for k in (3, 2, 1, 0):
        up_sum = exchanged(up_sum, "ep", k % 2, 2)
        down_sum = exchanged(down_sum, "ep", 1 - k % 2, 2)
        if k > 0:
            up_sum = whole_sum(up_sum, kept[k])
            down_sum = whole_sum(down_sum, kept[3 + k])
    expert_mix = whole_sum(up_sum, down_sum, kept[0])

    mixed_tokens = mixer(
        place,
        mixer_tokens,
        mixer_gain,
        in_weight,
        group_weight,
        channel_scale,
        out_weight,
        hidden_last,
    )
    return (mixed_tokens, expert_mix)


def solution(mesh):
    placed = (
        P(("grp", "ep", "tp"), None),
        P(),
        P(None, "tp"),
        P("tp", None, None),
        P("tp"),
        P("tp", None),
        P(("grp", "ep", "tp"), None),
        P(),
        P(("grp", "ep", "tp"), None),
        P(("grp", "ep", "tp"), None),
        P("ep", None, "tp"),
        P("ep", None, "tp"),
        P("ep", "tp", None),
    )

    return jax.shard_map(
        local,
        mesh=mesh,
        in_specs=placed,
        out_specs=(P(("grp", "ep", "tp"), None), P(("grp", "ep", "tp"), None)),
        check_vma=False,
    )
```

```python
import functools

import jax
import jax.numpy as jnp
from jax import lax
from jax.experimental import pallas as pl
from jax.experimental.pallas import tpu as pltpu
from jax.sharding import PartitionSpec as P


WINDOW_MAX = 16
META = 8
F32 = jnp.float32
BF16 = jnp.bfloat16


def shifted(value, axis, by):
    devices = lax.axis_size(axis)
    pairs = [(i, i + by) for i in range(devices) if 0 <= i + by < devices]
    return lax.ppermute(value, axis, pairs)


def exchanged(value, axis, phase, width=1):
    devices = lax.axis_size(axis)
    groups = devices // width
    pairs = []
    for i in range(devices):
        group, place = divmod(i, width)
        partner = (group + (1 if group % 2 == phase else -1)) % groups
        pairs.append((i, partner * width + place))
    return lax.ppermute(value, axis, pairs)


def exchanged_by_core(value, phase):
    sides, devices = lax.axis_size("ep"), lax.axis_size("tp")
    pairs = []
    for i in range(sides * devices):
        side, place = divmod(i, devices)
        partner = (place + (1 if place % 2 == (phase + side) % 2 else -1)) % devices
        pairs.append((i, side * devices + partner))
    return lax.ppermute(value, ("ep", "tp"), pairs)


def thrown(value, by):
    devices = lax.axis_size("ep")
    pairs = [(i, (i + (2 * by if i // 2 % 2 == 0 else -2 * by)) % devices) for i in range(devices)]
    return lax.ppermute(value, "ep", pairs)


def returned(value, by):
    return thrown(value, by if by % 2 else -by)


def opposite(value, axis):
    devices = lax.axis_size(axis)
    return lax.ppermute(value, axis, [(i, (i + devices // 2) % devices) for i in range(devices)])


def swapped(value, axis):
    devices = lax.axis_size(axis)
    return lax.ppermute(value, axis, [(i, i ^ 1) for i in range(devices)])


def call(mib, body, outs, *operands, scalars=1, waits=0, scratch=()):
    specs = (
        [pl.BlockSpec(memory_space=pltpu.SMEM)] * scalars
        + [pl.BlockSpec(memory_space=pltpu.VMEM)] * (len(operands) - scalars - waits)
        + [pl.BlockSpec(memory_space=pl.ANY)] * waits
    )
    return pl.pallas_call(
        body,
        out_shape=outs,
        in_specs=specs,
        out_specs=jax.tree.map(lambda _: pl.BlockSpec(memory_space=pltpu.VMEM), outs),
        scratch_shapes=list(scratch),
        compiler_params=pltpu.CompilerParams(vmem_limit_bytes=mib * 1024 * 1024),
    )(*operands)


def array(rows, width, dtype=BF16):
    return jax.ShapeDtypeStruct((rows, width), dtype)


def normalized(tokens_ref, gain_ref, out_ref, size=16):
    @pl.loop(0, tokens_ref.shape[0] // size)
    def _(i):
        here = pl.ds(pl.multiple_of(i * size, size), size)
        values = tokens_ref[here, :].astype(F32)
        scaled = values * lax.rsqrt(jnp.mean(values * values, axis=-1, keepdims=True) + 1e-06)
        out_ref[here, :] = (scaled * gain_ref[...].astype(F32)).astype(BF16)


def pack_body(ids_ref, weights_ref, tokens_ref, gain_ref, out_ref):
    rows, width = tokens_ref.shape
    normalized(tokens_ref, gain_ref, out_ref)
    weights = weights_ref[...]
    first, second = weights[0:1], weights[1:2]
    both = first + second
    lines = [ids_ref[0:1].astype(F32), ids_ref[1:2].astype(F32)]
    for share in (first / both, second / both):
        high = share.astype(BF16).astype(F32)
        lines += [high, share - high]
    lines += [jnp.zeros_like(first)] * (META - len(lines))
    meta = jnp.concatenate(lines, axis=0)
    meta = jnp.concatenate([meta, jnp.zeros((META, width - rows), F32)], axis=1)
    out_ref[rows:, :] = meta.astype(BF16)


def slots_of(block_ref, place_ref, chips, sign, count, capacity, kept):
    rows = block_ref.shape[0] - META
    meta = block_ref[rows:, 0:rows].astype(F32)
    chip, core = place_ref[0], place_ref[1]
    index = lax.broadcasted_iota(jnp.int32, (count, rows), 0)
    step = lax.shift_right_logical(index, 1)
    away = sign * (1 - 2 * (chip & 1))
    named = chip + away * (1 + step) + chips if sign else chip + 0 * step
    named = jnp.where(named >= chips, named - chips, named)
    named = jnp.where(named >= chips, named - chips, named)
    expert = (2 * named + ((core + (index & 1)) & 1)).astype(F32)
    is_first, is_second = meta[0:1] == expert, meta[1:2] == expert
    match = jnp.where(is_first, 1.0, 0.0) + jnp.where(is_second, 1.0, 0.0)
    shares = jnp.where(is_first, meta[2:3] + meta[3:4], 0.0) + jnp.where(
        is_second, meta[4:5] + meta[5:6], 0.0
    )
    upto = (
        lax.broadcasted_iota(jnp.int32, (rows, rows), 0)
        <= lax.broadcasted_iota(jnp.int32, (rows, rows), 1)
    ).astype(F32).astype(BF16)
    rank = jnp.dot(match.astype(BF16), upto, preferred_element_type=F32)
    slot = jnp.where(match > 0.5, rank - 1.0, -1.0)
    number = lax.broadcasted_iota(jnp.int32, (capacity, rows), 0).astype(F32)
    hot = [jnp.where(slot[e : e + 1] == number, 1.0, 0.0) for e in kept]
    return hot, [shares[e : e + 1] for e in kept]


def by_columns(width, body, pieces=8):
    @pl.loop(0, pieces)
    def _(i):
        body(pl.ds(pl.multiple_of(i * (width // pieces), 128), width // pieces))


def picked(chosen, block_ref, columns):
    rows = block_ref.shape[0] - META
    return jnp.dot(chosen, block_ref[0:rows, columns], preferred_element_type=F32).astype(BF16)


def weighed(hot, shares):
    values = [jnp.sum(h * s, axis=1, keepdims=True) for h, s in zip(hot, shares)]
    return jnp.concatenate(hot, axis=0).T.astype(BF16), values


def spread(chosen, values, results):
    scaled = [(v * r.astype(F32)).astype(BF16) for v, r in zip(values, results)]
    return jnp.dot(chosen, jnp.concatenate(scaled, axis=0), preferred_element_type=F32)


KEPT = {1: (0, 1, 2, 3, 4, 5, 6), -1: (0, 1, 2, 3, 4, 5, 7)}


def far_cuts(capacity):
    return [(2 * capacity * k, 2 * capacity * k + 2 * capacity) for k in range(3)] + [
        (6 * capacity, 7 * capacity)
    ]


def relay_body(chips, capacity, place_ref, up_ref, down_ref, *outs):
    todo = []
    for sign, block_ref, own in ((1, up_ref, outs[:4]), (-1, down_ref, outs[4:])):
        hot, _ = slots_of(block_ref, place_ref, chips, sign, 8, capacity, KEPT[sign])
        todo.append((jnp.concatenate(hot, axis=0).astype(BF16), block_ref, own))

    def piece(columns):
        for chosen, block_ref, own in todo:
            rows = picked(chosen, block_ref, columns)
            for (low, high), out_ref in zip(far_cuts(capacity), own):
                out_ref[:, columns] = rows[low:high]

    by_columns(up_ref.shape[1], piece)


def near_body(chips, capacity, place_ref, *refs):
    blocks, (same_ref, other_ref) = refs[:-2], refs[-2:]
    chosen = []
    for block_ref in blocks:
        hot, _ = slots_of(block_ref, place_ref, chips, 0, 8, capacity, (0, 1))
        chosen.append(jnp.concatenate(hot, axis=0).astype(BF16))

    def piece(columns):
        for i, block_ref in enumerate(blocks):
            rows = picked(chosen[i], block_ref, columns)
            same_ref[i * capacity : (i + 1) * capacity, columns] = rows[:capacity]
            other_ref[i * capacity : (i + 1) * capacity, columns] = rows[capacity:]

    by_columns(same_ref.shape[1], piece)


def unpack_body(capacity, near_ref, *refs):
    far, (same_ref, other_ref) = refs[:-2], refs[-2:]
    low = near_ref.shape[0]
    other_ref[0:low, :] = near_ref[...]
    for i in range(7):
        here = slice(i * capacity, (i + 1) * capacity)
        same_ref[here, :] = far[i][0:capacity, :]
    for i, k in enumerate((0, 1, 2, 4, 5, 6)):
        at = low + i * capacity
        other_ref[at : at + capacity, :] = far[k][capacity : 2 * capacity, :]
    other_ref[low + 6 * capacity :, :] = far[7][...]


def hidden_body(pairs, far_same, near_same, other, *refs):
    weights, out_ref, rows_ref = refs[: 2 * pairs], refs[-2], refs[-1]
    near, far = near_same.shape[0], far_same.shape[0]
    rows_ref[0:far, :] = far_same[...]
    rows_ref[far : 2 * far, :] = other[near:, :]
    rows_ref[2 * far : 2 * far + near, :] = near_same[...]
    rows_ref[2 * far + near :, :] = other[0:near, :]
    low = rows_ref.shape[0]

    @pl.loop(0, 4)
    def _(i):
        here = pl.ds(pl.multiple_of(i * (low // 4), 128), low // 4)
        for k in range(pairs):
            gate = jnp.dot(rows_ref[here, :], weights[2 * k][...], preferred_element_type=F32)
            upper = jnp.dot(rows_ref[here, :], weights[2 * k + 1][...], preferred_element_type=F32)
            made = (gate / (1.0 + jnp.exp(-gate)) * upper).astype(BF16)
            columns = made.shape[1]
            out_ref[here, k * columns : (k + 1) * columns] = made


def down_body(first, sizes, count, pieces, *refs):
    rows = sum(sizes)
    hidden = jnp.concatenate([ref[first : first + rows, :] for ref in refs[:count]], axis=1)
    outs = refs[len(refs) - len(sizes) :]
    weights = refs[count : len(refs) - len(sizes)]

    def piece(columns):
        total, low = 0.0, 0
        for ref in weights:
            total = total + jnp.dot(
                hidden[:, low : low + ref.shape[0]], ref[:, columns], preferred_element_type=F32
            )
            low += ref.shape[0]
        at = 0
        for size, out_ref in zip(sizes, outs):
            out_ref[:, columns] = total[at : at + size].astype(BF16)
            at += size

    by_columns(outs[0].shape[1], piece, pieces)


def far_back_body(capacity, same_ref, other_ref, *outs):
    for i in range(3):
        for base, own in ((0, outs[:4]), (4, outs[4:])):
            j = i + base
            k = i if base == 0 else i + 3
            own[i][0:capacity, :] = same_ref[j * capacity : (j + 1) * capacity, :]
            own[i][capacity:, :] = other_ref[k * capacity : (k + 1) * capacity, :]
    outs[3][...] = same_ref[3 * capacity : 4 * capacity, :]
    outs[7][...] = other_ref[6 * capacity : 7 * capacity, :]


def own_weighed(block_ref, place_ref, chips, capacity):
    return weighed(*slots_of(block_ref, place_ref, chips, 0, 8, capacity, (0, 1)))


def own_part(made, i, capacity, same_ref, other_ref, columns):
    low, high = i * capacity, (i + 1) * capacity
    return spread(*made, [same_ref[low:high, columns], other_ref[low:high, columns]])


def turn_body(chips, capacity, at, place_ref, up_ref, down_ref, same_ref, other_ref, *refs):
    far, outs = refs[:8], refs[8:]
    todo = []
    for sign, block_ref, own, i, out_ref in (
        (1, up_ref, far[:4], at[0], outs[0]),
        (-1, down_ref, far[4:], at[1], outs[1]),
    ):
        made = weighed(*slots_of(block_ref, place_ref, chips, sign, 8, capacity, KEPT[sign]))
        near = own_weighed(block_ref, place_ref, chips, capacity)
        todo.append((made, near, own, i, out_ref))

    def piece(columns):
        for made, near, own, i, out_ref in todo:
            results = []
            for ref in own:
                for low in range(0, ref.shape[0], capacity):
                    results.append(ref[low : low + capacity, columns])
            total = spread(*made, results)
            total = total + own_part(near, i, capacity, same_ref, other_ref, columns)
            out_ref[:, columns] = total.astype(BF16)

    by_columns(up_ref.shape[1], piece)


def near_back_body(chips, capacity, count, place_ref, *refs):
    blocks = refs[:count]
    same_ref, other_ref = refs[count : count + 2]
    outs = refs[count + 2 :]
    near = [own_weighed(block_ref, place_ref, chips, capacity) for block_ref in blocks]

    def piece(columns):
        for i, out_ref in enumerate(outs):
            total = own_part(near[i], i, capacity, same_ref, other_ref, columns)
            out_ref[:, columns] = total.astype(BF16)

    by_columns(same_ref.shape[1], piece, 16)


def mixer_norm_body(tokens_ref, gain_ref, _, out_ref):
    normalized(tokens_ref, gain_ref, out_ref)


def ring_of_four(me):
    return me, me + 1 - 2 * (me & 1), 3 - me, (me + 2) & 3


def mixer_first_body(place_ref, *refs):
    blocks, weight_ref, out_ref, held_ref = refs[:4], *refs[4:]
    rows = blocks[0].shape[0]
    for block_ref, place in zip(blocks, ring_of_four(place_ref[2])):
        held_ref[pl.ds(pl.multiple_of(place * rows, rows), rows), :] = block_ref[...]

    @pl.loop(0, 4)
    def _(i):
        here = pl.ds(pl.multiple_of(i * rows, rows), rows)
        made = jnp.dot(held_ref[here, :], weight_ref[...], preferred_element_type=F32)
        out_ref[here, :] = made.astype(BF16)


def mixer_second_body(place_ref, rim_ref, rows_ref, group_ref, scale_ref, weight_ref, *refs):
    outs, extended_ref = refs[:4], refs[4]
    rim, total = rim_ref.shape[0], rows_ref.shape[0]
    rows = total // 4
    extended_ref[0:rim, :] = rim_ref[...]
    extended_ref[rim:, :] = rows_ref[...]
    window = lax.shift_left(jnp.int32(2), place_ref[2])
    behind = (
        lax.broadcasted_iota(jnp.int32, (rows, rows + rim), 0)
        - lax.broadcasted_iota(jnp.int32, (rows, rows + rim), 1)
        + rim
    )
    inside = jnp.where((behind >= 0) & (behind < window), 1.0, 0.0).astype(BF16)
    grouped = []
    for place in ring_of_four(place_ref[2]):
        at = pl.multiple_of(place * rows, rows)
        values = rows_ref[pl.ds(at, rows), :].astype(F32)
        sums = jnp.dot(
            inside, extended_ref[pl.ds(at, rows + rim), :], preferred_element_type=F32
        )
        position = place_ref[3] * total + at + 1 + lax.broadcasted_iota(jnp.int32, (rows, 1), 0)
        counts = jnp.minimum(position, window).astype(F32)
        pooled = (sums / counts - values).astype(BF16)
        made = jnp.dot(pooled, group_ref[...], preferred_element_type=F32)
        grouped.append((made * scale_ref[...].astype(F32)).astype(BF16))
    grouped = jnp.concatenate(grouped, axis=0)

    def piece(columns):
        made = jnp.dot(grouped, weight_ref[:, columns], preferred_element_type=F32).astype(BF16)
        for k, out_ref in enumerate(outs):
            out_ref[:, columns] = made[k * rows : (k + 1) * rows]

    by_columns(weight_ref.shape[1], piece)


def sum_body(*refs):
    planes, out_ref = [], refs[-1]
    for ref in refs[:-1]:
        planes += [ref] if len(ref.shape) == 2 else [ref.at[i] for i in range(ref.shape[0])]
    pieces = 8
    rows = out_ref.shape[0] // pieces

    @pl.loop(0, pieces)
    def _(i):
        here = pl.ds(pl.multiple_of(i * rows, rows), rows)
        total = planes[0][here, :].astype(F32)
        for ref in planes[1:]:
            total = total + ref[here, :].astype(F32)
        out_ref[here, :] = total.astype(BF16)


def whole_sum(*values):
    return call(6, sum_body, array(*values[0].shape[-2:]), *values, scalars=0)


def around(here, first, second, across):
    return [here, exchanged(first, "tp", 0), exchanged(second, "tp", 1), opposite(across, "tp")]


def mixer(
    place, mixer_tokens, mixer_gain, in_weight, group_weight, channel_scale, out_weight, wait
):
    rows, width = mixer_tokens.shape
    members = lax.axis_size("tp")
    columns = in_weight.shape[1]
    normed = call(
        6,
        mixer_norm_body,
        array(rows, width),
        mixer_tokens,
        mixer_gain[None],
        wait,
        scalars=0,
        waits=1,
    )
    blocks = around(normed, normed, normed, normed)
    pooled_in = call(
        12,
        mixer_first_body,
        array(rows * members, columns),
        place,
        *blocks,
        in_weight,
        scratch=[pltpu.VMEM((rows * members, width), BF16)],
    )
    rim = shifted(pooled_in[rows * members - WINDOW_MAX :], "ep", 1)
    parts = call(
        16,
        mixer_second_body,
        [array(rows, width)] * members,
        place,
        rim,
        pooled_in,
        group_weight[0],
        channel_scale[None],
        out_weight,
        scratch=[pltpu.VMEM((rows * members + WINDOW_MAX, columns), BF16)],
    )
    parts = around(*parts)
    return whole_sum(*parts)


def local(
    mixer_tokens,
    mixer_gain,
    in_weight,
    group_weight,
    channel_scale,
    out_weight,
    expert_tokens,
    expert_gain,
    route_ids,
    route_weights,
    gate_weight,
    up_weight,
    down_weight,
):
    rows, width = expert_tokens.shape
    chips = lax.axis_size("ep") // 2
    capacity = 4 * rows // (2 * chips)
    side = lax.axis_index("ep")
    place = jnp.stack([side >> 1, side & 1, lax.axis_index("tp"), side]).astype(jnp.int32)
    block_rows = rows + META

    gates, uppers = gate_weight[0], up_weight[0]
    gate_pair = [exchanged_by_core(gates, phase) for phase in (0, 1)]
    upper_pair = [exchanged_by_core(uppers, phase) for phase in (0, 1)]
    down_pair = [exchanged_by_core(down_weight[0], phase) for phase in (0, 1)]
    gate_last = exchanged_by_core(gate_pair[1], 0)
    upper_last = exchanged_by_core(upper_pair[0], 1)
    down_last = exchanged_by_core(down_pair[1], 0)

    block = call(
        6,
        pack_body,
        array(block_rows, width),
        route_ids.T,
        route_weights.T,
        expert_tokens,
        expert_gain[None],
        scalars=0,
    )
    ups, downs = [block], [block]
    for k in range(4):
        ups.append(exchanged(ups[-1], "ep", k % 2, 2))
        downs.append(exchanged(downs[-1], "ep", 1 - k % 2, 2))
    pieces = [array(high - low, width) for low, high in far_cuts(capacity)]
    far = call(
        8, functools.partial(relay_body, chips, capacity), pieces * 2, place, ups[4], downs[4]
    )
    far = [thrown(far[k], k + 1) for k in range(4)] + [
        thrown(far[4 + k], -(k + 1)) for k in range(4)
    ]
    blocks = [block] + ups[1:4] + downs[1:4] + [ups[4], downs[4]]
    near_same, near_other = call(
        12,
        functools.partial(near_body, chips, capacity),
        [array(9 * capacity, width)] * 2,
        place,
        *blocks,
    )
    far_same, other = call(
        6,
        functools.partial(unpack_body, capacity),
        [array(7 * capacity, width), array(16 * capacity, width)],
        near_other,
        *far,
        scalars=0,
    )
    other = swapped(other, "ep")

    parts = [far_same, near_same, other]
    sizes = [7 * capacity] * 2 + [9 * capacity] * 2
    total = sum(sizes)
    ff = gates.shape[1]
    rows_scratch = [pltpu.VMEM((total, width), BF16)]
    hidden = call(
        24,
        functools.partial(hidden_body, 3),
        array(total, 3 * ff),
        *parts,
        gates,
        uppers,
        gate_pair[0],
        upper_pair[0],
        gate_pair[1],
        upper_pair[1],
        scalars=0,
        scratch=rows_scratch,
    )
    hidden_last = call(
        16,
        functools.partial(hidden_body, 1),
        array(total, ff),
        *parts,
        gate_last,
        upper_last,
        hidden,
        scalars=0,
        waits=1,
        scratch=rows_scratch,
    )

    def results(first, sizes):
        return call(
            16,
            functools.partial(down_body, first, sizes, 2, 16 if first else 8),
            [array(size, width) for size in sizes],
            hidden,
            hidden_last,
            down_weight[0],
            *down_pair,
            down_last,
            scalars=0,
        )

    far_same, far_other = results(0, sizes[:2])
    near_same, near_other = results(sum(sizes[:2]), sizes[2:])

    far_other = swapped(far_other, "ep")
    near_other = swapped(near_other, "ep")
    back = call(
        6, functools.partial(far_back_body, capacity), pieces * 2, far_same, far_other, scalars=0
    )
    back = [returned(back[k], k + 1) for k in range(4)] + [
        returned(back[4 + k], -(k + 1)) for k in range(4)
    ]
    kept = call(
        16,
        functools.partial(near_back_body, chips, capacity, 7),
        [array(rows, width)] * 7,
        place,
        *blocks[:7],
        near_same,
        near_other,
    )
    up_sum, down_sum = call(
        10,
        functools.partial(turn_body, chips, capacity, (7, 8)),
        [array(rows, width)] * 2,
        place,
        ups[4],
        downs[4],
        near_same,
        near_other,
        *back,
    )
    for k in (3, 2, 1, 0):
        up_sum = exchanged(up_sum, "ep", k % 2, 2)
        down_sum = exchanged(down_sum, "ep", 1 - k % 2, 2)
        if k > 0:
            up_sum = whole_sum(up_sum, kept[k])
            down_sum = whole_sum(down_sum, kept[3 + k])
    expert_mix = whole_sum(up_sum, down_sum, kept[0])

    mixed_tokens = mixer(
        place,
        mixer_tokens,
        mixer_gain,
        in_weight,
        group_weight,
        channel_scale,
        out_weight,
        hidden_last,
    )
    return (mixed_tokens, expert_mix)


def solution(mesh):
    placed = (
        P(("grp", "ep", "tp"), None),
        P(),
        P(None, "tp"),
        P("tp", None, None),
        P("tp"),
        P("tp", None),
        P(("grp", "ep", "tp"), None),
        P(),
        P(("grp", "ep", "tp"), None),
        P(("grp", "ep", "tp"), None),
        P("ep", None, "tp"),
        P("ep", None, "tp"),
        P("ep", "tp", None),
    )

    return jax.shard_map(
        local,
        mesh=mesh,
        in_specs=placed,
        out_specs=(P(("grp", "ep", "tp"), None), P(("grp", "ep", "tp"), None)),
        check_vma=False,
    )
```
